32 devices in a mesh: ep: 8 (over z, x), tp: 4 (over y, core).
Axes of the slice: x: 2, y: 2, z: 4, core: 2. Of those that a mesh axis runs over, the one named last changes fastest.
Arguments:
- tokens: bfloat16 [256, 2048], P('ep'), may hold values from -24 to 24
- norm_gain: float32 [2048], replicated, may hold values from 0.1 to 1.9
- post_gain: float32 [2048], replicated, may hold values from 0.1 to 1.9
- w_query: bfloat16 [2048, 2048], P(None, 'tp'), may hold values from -0.125 to 0.125
- w_key: bfloat16 [2048, 512], P(None, 'tp'), may hold values from -0.125 to 0.125
- w_value: bfloat16 [2048, 512], P(None, 'tp'), may hold values from -0.125 to 0.125
- w_forget: bfloat16 [2048, 32], replicated, may hold values from -0.25 to 0.25
- w_output: bfloat16 [2048, 2048], P('tp'), may hold values from -0.125 to 0.125
- key_cache: bfloat16 [256, 8, 64, 1024], P('ep', 'tp'), may hold values from -660 to 660
- value_cache: bfloat16 [256, 8, 64, 1024], P('ep', 'tp'), may hold values from -6 to 6
- gate_cache: float32 [256, 32, 1024], P('ep', 'tp'), may hold values from -176.08 to 0, as said below
- lengths: int32 [256], P('ep'), may hold values from 256 to 1024
- routes: int32 [256, 2], P('ep'), may hold values from 0 to 7, all different within a row; in each aligned block of 32 rows (0 to 31, 32 to 63, ...) at most 16 rows name the same one
- route_logits: float32 [256, 2], P('ep'), may hold values from -6 to 6
- w_gate: bfloat16 [8, 2048, 3584], P('ep', None, 'tp'), may hold values from -0.125 to 0.125
- w_up: bfloat16 [8, 2048, 3584], P('ep', None, 'tp'), may hold values from -0.125 to 0.125
- w_down: bfloat16 [8, 3584, 2048], P('ep', 'tp'), may hold values from -0.09375 to 0.09375
Outputs:
- layer_out: bfloat16 [256, 2048], P('ep', 'tp')
The draws below stay inside these ranges and needn't reach their ends.
Inputs may be any that keep to these rules, and one draw needn't show every extreme that they name: `routes`: each row names 2 different experts. The rows of one index of ep name any one expert at most 16 times, and in every draw some index of ep names some expert exactly 16 times. `gate_cache`: cumulative sums of negative log forget gates along positions: nonincreasing along the last dimension. `lengths`: the new token follows the valid positions of its sequence.
All inputs are finite; a program needn't handle non-finite values.
Results may differ from the reference program's by a relative error of at most 0.011.
Values may be sent and summed in bfloat16 or wider, within the bound.
No kernel may reach another device: no remote copies, remote signals or barrier semaphores. Data moves between devices by JAX's collectives and lax.ppermute only.
A program may use at most 64 MiB of HBM per device.

```python
import math
import jax
import jax.numpy as jnp
import numpy as np
from jax import lax

WIDTH = 2048
QUERY_HEADS = 32
HEAD_DIM = 64
KV_HEADS = 8
FFN = 3584
TOPK = 2
TOK_GRP = 32
CACHE_POSITIONS = 1024
SEQUENCE_TOTAL = 256
EXPERTS = 8
CAP = 16
N_EP = 8
N_TP = 4


def draw_tokens(key, part):
    first, second = jax.random.split(jax.random.fold_in(key, 3))
    row_scale = jnp.exp(jax.random.uniform(first, (SEQUENCE_TOTAL, 1), jnp.float32, jnp.log(0.3), jnp.log(3.0)))
    column_scale = 0.4 * jnp.exp(jnp.log(4.0) * jnp.arange(WIDTH, dtype=jnp.float32) / WIDTH)
    base = jnp.clip(jax.random.normal(second, (SEQUENCE_TOTAL, WIDTH), jnp.float32), -5.0, 5.0)
    return (row_scale * column_scale[None, :] * base).astype(jnp.bfloat16)


def draw_key_cache(key, part):
    first = jax.random.fold_in(jax.random.fold_in(key, 5), 0)
    base = jnp.clip(jax.random.normal(first, (SEQUENCE_TOTAL, KV_HEADS, HEAD_DIM, CACHE_POSITIONS), jnp.float32), -6.0, 6.0)
    return base.astype(jnp.bfloat16)


def draw_gate_cache(key, part):
    key_entries = jax.random.split(jax.random.fold_in(key, 7), 7)
    slow_share = 0.5
    keeps = jax.random.uniform(key_entries[0], (SEQUENCE_TOTAL, QUERY_HEADS, 1), jnp.float32) < slow_share
    slow_total = jax.random.uniform(key_entries[1], (SEQUENCE_TOTAL, QUERY_HEADS, 1), jnp.float32, 0.2, 0.9)
    fast_rate = jnp.exp(jax.random.uniform(key_entries[2], (SEQUENCE_TOTAL, QUERY_HEADS, 1), jnp.float32, jnp.log(0.03), jnp.log(0.1)))
    decay_rate = jnp.where(keeps, slow_total / CACHE_POSITIONS, fast_rate)
    coarse_estimate = jax.random.uniform(key_entries[3], (SEQUENCE_TOTAL, QUERY_HEADS, CACHE_POSITIONS), jnp.float32, 0.3, 1.7)
    cache_position = jnp.arange(CACHE_POSITIONS, dtype=jnp.int32)[None, None, :]
    leading_group = jax.random.randint(key_entries[4], (SEQUENCE_TOTAL, QUERY_HEADS, 1), 0, CACHE_POSITIONS)
    trailing_group = jax.random.randint(key_entries[5], (SEQUENCE_TOTAL, QUERY_HEADS, 1), 0, CACHE_POSITIONS)
    group_length = jax.random.uniform(key_entries[6], (SEQUENCE_TOTAL, QUERY_HEADS, 2), jnp.float32, 0.22, 0.69)
    position_groups = (cache_position == leading_group).astype(jnp.float32) * group_length[:, :, 0:1] + (cache_position == trailing_group).astype(jnp.float32) * group_length[:, :, 1:2]
    decode_steps = -decay_rate * coarse_estimate - position_groups
    return jnp.cumsum(decode_steps, axis=-1).astype(jnp.float32)


def with_ends(entries, rng, least, high):
    index_at = [jax.random.randint(jax.random.fold_in(rng, axis), (), 0, length) for axis, length in enumerate(entries.shape)]
    widest = entries.shape.index(max(entries.shape))
    beside = index_at[:widest] + [(index_at[widest] + 1) % entries.shape[widest]] + index_at[widest + 1:]
    return entries.at[tuple(index_at)].set(least).at[tuple(beside)].set(high)


def block_levels(stream_key, extent, cuts, low, largest):
    loudness, own = 1.0, jax.random.fold_in(stream_key, 6)
    for position, blocks in cuts:
        draws = jnp.exp(jax.random.uniform(jax.random.fold_in(own, position), (blocks,), jnp.float32, low / len(cuts), largest / len(cuts)))
        loudness = loudness * jnp.repeat(draws, extent[position] // blocks).reshape([-1 if axis == position else 1 for axis in range(len(extent))])
    return loudness


def assign_block(key, own, number, rows, count, top, bound, lean):
    ranking = jax.random.permutation(key, count)
    crowded, ordinary = load_shares(count, rows * top, bound, lean, True), load_shares(count, rows * top, bound, lean, False)
    places = jnp.arange(count)

    def named(sizes, rotation):
        used = int((sizes > 0).sum())
        fixed = max(1, used // 4)
        moved = fixed + (places - fixed + rotation * (used - fixed)) % max(1, count - fixed)
        return jnp.zeros((count,), jnp.int32).at[ranking[jnp.where(places < fixed, places, moved)]].set(jnp.asarray(sizes, jnp.int32))

    sizes = jnp.where(number % 4 == 0, named(crowded, number // 4), named(ordinary, number - number // 4 - 1))
    mixed = jax.random.permutation(jax.random.fold_in(own, 3), count)
    giver, receiver = mixed[0:count // 2 * 2:2], mixed[1:count // 2 * 2:2]
    slack = jnp.minimum(sizes[giver] - 1, bound - sizes[receiver]) // 2
    slack = jnp.where((giver == ranking[0]) | (receiver == ranking[0]) | (sizes[receiver] == 0), 0, jnp.maximum(slack, 0))
    moved = jax.random.randint(jax.random.fold_in(own, 4), (count // 2,), 0, 1 << 20) % (slack + 1)
    sizes = sizes.at[giver].add(-moved).at[receiver].add(moved)
    labels = jnp.searchsorted(jnp.cumsum(sizes), jnp.arange(rows * top), side="right").astype(jnp.int32)
    listing = labels.reshape(top, rows).T
    listing = listing[jax.random.permutation(jax.random.fold_in(own, 1), rows)]
    rotation = jax.random.randint(jax.random.fold_in(own, 2), (rows, 1), 0, top)
    return jnp.take_along_axis(listing, (jnp.arange(top)[None, :] + rotation) % top, axis=1)


def load_shares(count, total, most, lean, full):
    portions = [(1 << 20) // math.isqrt(grade ** lean) + 1 for grade in range(1, count + 1)]
    largest = most if full else min(most, max(-(-total // count), total * portions[0] // sum(portions)))
    least = 1 if total - largest >= count - 1 else 0
    holding, rest = [largest] + [least] * (count - 1), total - largest - least * (count - 1)
    while rest > 0:
        candidates = [i for i in range(1, count) if holding[i] < largest] or [i for i in range(1, count) if holding[i] < most]
        mass, remaining = sum([portions[i] for i in candidates]), rest
        for i in candidates:
            more = min(most - holding[i], max(1, remaining * portions[i] // mass), rest)
            holding[i] = holding[i] + more
            rest = rest - more
    return np.array(holding)


def bell_draw(rng, extent, scale, bound, shards=(), kind=jnp.bfloat16):
    values = jax.random.normal(rng, extent, jnp.float32) * scale
    if len(shards) > 0:
        values = block_levels(rng, extent, shards, -0.22, 0.18) * values
    return jnp.clip(values, min=-bound, max=bound).astype(kind)


def setup_inputs(seed: int = 0) -> dict:
    seeds = jax.random.split(jax.random.key(seed), 18)
    tokens = draw_tokens(jax.random.fold_in(seeds[17], 71), 0)
    norm_gain = jnp.clip(1.0 + 0.18 * jax.random.normal(seeds[1], (WIDTH,), jnp.float32), 0.1, 1.9)
    post_gain = jnp.clip(1.0 + 0.18 * jax.random.normal(seeds[2], (WIDTH,), jnp.float32), 0.1, 1.9)
    w_query = bell_draw(seeds[3], (WIDTH, QUERY_HEADS * HEAD_DIM), WIDTH ** -0.5, 0.125, ((1, 4),))
    w_key = bell_draw(seeds[4], (WIDTH, KV_HEADS * HEAD_DIM), WIDTH ** -0.5, 0.125, ((1, 4),))
    w_value = bell_draw(seeds[5], (WIDTH, KV_HEADS * HEAD_DIM), WIDTH ** -0.5, 0.125, ((1, 4),))
    w_forget = bell_draw(seeds[6], (WIDTH, QUERY_HEADS), (WIDTH // 4) ** -0.5, 0.25)
    w_output = bell_draw(seeds[7], (QUERY_HEADS * HEAD_DIM, WIDTH), (QUERY_HEADS * HEAD_DIM) ** -0.5, 0.125, ((0, 4),))
    key_cache = draw_key_cache(jax.random.fold_in(seeds[17], 71), 0)
    value_cache = bell_draw(seeds[9], (SEQUENCE_TOTAL, KV_HEADS, HEAD_DIM, CACHE_POSITIONS), 1.0, 6.0, ((0, 8), (1, 4)))
    gate_cache = draw_gate_cache(jax.random.fold_in(seeds[17], 71), 0)
    lengths = with_ends(jax.random.randint(seeds[11], (SEQUENCE_TOTAL,), CACHE_POSITIONS // 4, CACHE_POSITIONS + 1), jax.random.fold_in(seeds[11], 1), CACHE_POSITIONS // 4, CACHE_POSITIONS).astype(jnp.int32)
    routes_keys = jax.random.split(jax.random.fold_in(seeds[12], 1), SEQUENCE_TOTAL // TOK_GRP)
    routes_turns = jax.random.permutation(jax.random.fold_in(seeds[12], 3), SEQUENCE_TOTAL // TOK_GRP)
    routes = jax.vmap(lambda own, number: assign_block(jax.random.fold_in(seeds[12], 2), own, number, TOK_GRP, EXPERTS, TOPK, CAP, 2))(routes_keys, routes_turns).reshape((SEQUENCE_TOTAL, TOPK))
    route_logits = bell_draw(seeds[13], (SEQUENCE_TOTAL, TOPK), 1.5, 6.0, ((0, 8),), jnp.float32)
    w_gate = bell_draw(seeds[14], (EXPERTS, WIDTH, FFN), WIDTH ** -0.5, 0.125, ((0, 8), (2, 4)))
    w_up = bell_draw(seeds[15], (EXPERTS, WIDTH, FFN), WIDTH ** -0.5, 0.125, ((0, 8), (2, 4)))
    w_down = bell_draw(seeds[16], (EXPERTS, FFN, WIDTH), FFN ** -0.5, 0.09375, ((0, 8), (1, 4)))
    return dict(tokens=tokens, norm_gain=norm_gain, post_gain=post_gain, w_query=w_query, w_key=w_key, w_value=w_value, w_forget=w_forget, w_output=w_output, key_cache=key_cache, value_cache=value_cache, gate_cache=gate_cache, lengths=lengths, routes=routes, route_logits=route_logits, w_gate=w_gate, w_up=w_up, w_down=w_down)


epsilon = 1e-06

def normalize(rows, gain):
    return rows * lax.rsqrt(lax.optimization_barrier(jnp.mean(rows * rows, axis=-1, keepdims=True)) + epsilon) * gain

def attend_one(packed):
    query_vector, fresh_key, value_new, log_forget, key_rows, value_rows, gates, length = packed
    group_size = QUERY_HEADS // KV_HEADS
    score_scale = HEAD_DIM ** (-0.5)
    grouped = query_vector.reshape(KV_HEADS, group_size, HEAD_DIM).astype(jnp.float32)
    past_scores = jnp.einsum('kgd,kdl->kgl', grouped, key_rows.astype(jnp.float32)).reshape(QUERY_HEADS, CACHE_POSITIONS)
    cache_position = jnp.arange(CACHE_POSITIONS, dtype=jnp.int32)[None, :]
    latest = lax.optimization_barrier(jnp.sum(jnp.where(cache_position == length - 1, gates, 0.0), axis=-1))
    past_scores = past_scores * score_scale + (latest + log_forget)[:, None] - gates
    past_scores = jnp.where(cache_position < length, past_scores, -jnp.inf)
    new_score = jnp.einsum('kgd,kd->kg', grouped, fresh_key.astype(jnp.float32)).reshape(QUERY_HEADS) * score_scale
    peak_score = jnp.maximum(lax.optimization_barrier(jnp.max(past_scores, axis=-1)), new_score)
    past_exp = jnp.exp(past_scores - peak_score[:, None])
    new_exp = jnp.exp(new_score - peak_score)
    denominator = lax.optimization_barrier(jnp.sum(past_exp, axis=-1)) + new_exp
    past_prob = (past_exp / denominator[:, None]).astype(jnp.bfloat16)
    new_prob = (new_exp / denominator).astype(jnp.bfloat16)
    mixed = jnp.einsum('kgl,kdl->kgd', past_prob.reshape(KV_HEADS, group_size, CACHE_POSITIONS).astype(jnp.float32), value_rows.astype(jnp.float32))
    mixed = mixed + new_prob.reshape(KV_HEADS, group_size)[:, :, None].astype(jnp.float32) * value_new[:, None, :].astype(jnp.float32)
    return mixed.reshape(QUERY_HEADS * HEAD_DIM).astype(jnp.bfloat16)

def reference(tokens, norm_gain, post_gain, w_query, w_key, w_value, w_forget, w_output, key_cache, value_cache, gate_cache, lengths, routes, route_logits, w_gate, w_up, w_down):
    tokens_wide = tokens.astype(jnp.float32)
    normed = normalize(tokens_wide, norm_gain).astype(jnp.bfloat16)
    query_vector = jnp.dot(normed, w_query, preferred_element_type=jnp.float32).astype(jnp.bfloat16)
    fresh_key = jnp.dot(normed, w_key, preferred_element_type=jnp.float32).astype(jnp.bfloat16)
    value_new = jnp.dot(normed, w_value, preferred_element_type=jnp.float32).astype(jnp.bfloat16)
    log_forget = jax.nn.log_sigmoid(jnp.dot(normed, w_forget, preferred_element_type=jnp.float32))
    attended = lax.map(attend_one, (query_vector, fresh_key.reshape(SEQUENCE_TOTAL, KV_HEADS, HEAD_DIM), value_new.reshape(SEQUENCE_TOTAL, KV_HEADS, HEAD_DIM), log_forget, key_cache, value_cache, gate_cache, lengths))
    head_block = QUERY_HEADS * HEAD_DIM // N_TP
    blocks = attended.reshape(SEQUENCE_TOTAL, N_TP, head_block).transpose(1, 0, 2).astype(jnp.float32)
    parts = jnp.einsum('tsr,trw->tsw', blocks, w_output.reshape(N_TP, head_block, WIDTH).astype(jnp.float32))
    attention = lax.optimization_barrier(jnp.sum(parts.astype(jnp.bfloat16).astype(jnp.float32), axis=0))
    stream = tokens_wide + attention
    expert_input = normalize(stream, post_gain).astype(jnp.bfloat16)
    route_count = SEQUENCE_TOTAL * TOPK
    per_expert = CAP * N_EP
    flat_routes = routes.reshape(route_count)
    expert_onehot = (flat_routes[:, None] == jnp.arange(EXPERTS, dtype=jnp.int32)[None, :]).astype(jnp.int32)
    route_rank = lax.optimization_barrier(jnp.sum(jnp.cumsum(expert_onehot, axis=0) * expert_onehot, axis=1)) - 1
    slot_index = (flat_routes * per_expert + route_rank).astype(jnp.int32)
    slot_token = jnp.zeros((EXPERTS * per_expert,), jnp.int32).at[slot_index].set(jnp.arange(route_count, dtype=jnp.int32) // TOPK)
    ff_block = FFN // N_TP

    def run_expert(index):
        chosen = lax.dynamic_slice_in_dim(slot_token, (index * per_expert).astype(jnp.int32), per_expert)
        expert_rows = expert_input[chosen]
        gate_act = jnp.dot(expert_rows, w_gate[index], preferred_element_type=jnp.float32)
        upper = jnp.dot(expert_rows, w_up[index], preferred_element_type=jnp.float32)
        hidden_act = (jax.nn.silu(gate_act) * upper).astype(jnp.bfloat16)
        down_parts = jnp.einsum('rtf,tfw->trw', hidden_act.reshape(per_expert, N_TP, ff_block).astype(jnp.float32), w_down[index].reshape(N_TP, ff_block, WIDTH).astype(jnp.float32))
        return lax.optimization_barrier(jnp.sum(down_parts.astype(jnp.bfloat16).astype(jnp.float32), axis=0)).astype(jnp.bfloat16)
    outputs = lax.map(run_expert, jnp.arange(EXPERTS, dtype=jnp.int32))
    picked = outputs.reshape(EXPERTS * per_expert, WIDTH)[slot_index].astype(jnp.float32).reshape(SEQUENCE_TOTAL, TOPK, WIDTH)
    route_weight = jax.nn.softmax(route_logits, axis=-1)
    expert_mix = lax.optimization_barrier(jnp.sum(route_weight[:, :, None] * picked, axis=1))
    return (stream + expert_mix).astype(jnp.bfloat16)
```

```python
import functools

import jax
import jax.numpy as jnp
from jax import lax
from jax.experimental import pallas as pl
from jax.experimental.pallas import tpu as pltpu
from jax.sharding import Mesh
from jax.sharding import PartitionSpec as P

epsilon = 1e-06
CORES = 2
F32 = jnp.float32
BF16 = jnp.bfloat16
NT = (((1,), (1,)), ((), ()))


def log2(n):
    assert n & (n - 1) == 0
    return n.bit_length() - 1


def dot(a, b):
    return jnp.dot(a, b, preferred_element_type=F32)


def iota(shape, axis):
    return lax.broadcasted_iota(jnp.int32, shape, axis)


def attention_kernel(
    sizes,
    where_ref,
    lengths_ref,
    tokens_hbm,
    gain_hbm,
    forget_hbm,
    query_hbm,
    key_w_hbm,
    value_w_hbm,
    out_w_hbm,
    key_hbm,
    value_hbm,
    gate_hbm,
    routes_ref,
    logits_ref,
    keep_ref,
    send_ref,
    dispatch_ref,
    combine_ref,
    tokens_ref,
    gain_ref,
    forget_ref,
    query_w,
    key_w,
    value_w,
    out_w,
    keys,
    values,
    gates,
    wide_query,
    mixed,
    forget_col,
    new_col,
    new_value,
    first_sems,
    cache_sems,
):
    seqs, heads, kv, head_dim, span, group, y_count, ep_count, capacity = sizes
    groups = seqs // group
    rows = group * heads
    kv_width = kv * head_dim
    head_width = heads * head_dim
    firsts = [
        (tokens_hbm, tokens_ref),
        (gain_hbm, gain_ref),
        (forget_hbm, forget_ref),
        (query_hbm, query_w),
        (key_w_hbm, key_w),
        (value_w_hbm, value_w),
        (out_w_hbm, out_w),
    ]
    copies = [
        pltpu.make_async_copy(src, dst, first_sems.at[i]) for i, (src, dst) in enumerate(firsts)
    ]

    caches = ((key_hbm, keys), (gate_hbm, gates), (value_hbm, values))

    def cache_copy(g, i):
        part = pl.ds(g * group, group)
        src, dst = caches[i]
        return pltpu.make_async_copy(src.at[part], dst.at[part], cache_sems.at[g, i])

    for c in copies[:-1]:
        c.start()
    for g in range(groups):
        for i in range(3):
            cache_copy(g, i).start()
    copies[-1].start()

    core = where_ref[0]
    head_start = where_ref[1]

    experts = iota((ep_count, seqs), 0)
    picks = [routes_ref[k : k + 1, :] for k in range(2)]
    named = jnp.zeros((ep_count, seqs), F32)
    for k in range(2):
        named = named + (experts == picks[k]).astype(F32)
    earlier = (iota((seqs, seqs), 0) < iota((seqs, seqs), 1)).astype(BF16)
    rank = dot(named.astype(BF16), earlier)
    slot_of = experts.astype(F32) * capacity + rank
    slots = [
        jnp.sum(jnp.where(experts == picks[k], slot_of, 0.0), axis=0, keepdims=True)
        for k in range(2)
    ]
    slot_iota = iota((ep_count * capacity, seqs), 0).astype(F32)
    dispatch_ref[...] = jnp.logical_or(slot_iota == slots[0], slot_iota == slots[1]).astype(
        F32
    ).astype(BF16)
    logits = [logits_ref[k : k + 1, :] for k in range(2)]
    top = jnp.maximum(logits[0], logits[1])
    raised = [jnp.exp(x - top) for x in logits]
    total = raised[0] + raised[1]
    eye = iota((seqs, seqs), 0) == iota((seqs, seqs), 1)

    def column(x):
        return jnp.sum(jnp.where(eye, x, 0.0), axis=1, keepdims=True)

    returned = (seqs, ep_count * y_count * capacity)
    back = iota(returned, 1)
    back_slot = (
        lax.shift_right_logical(back, log2(y_count * capacity)) * capacity
        + jnp.bitwise_and(back, capacity - 1)
    ).astype(F32)
    combine_ref[...] = jnp.where(
        back_slot == column(slots[0]), column(raised[0] / total), 0.0
    ) + jnp.where(back_slot == column(slots[1]), column(raised[1] / total), 0.0)

    for c in copies[:2]:
        c.wait()
    wide = tokens_ref[...].astype(F32)
    normed = (
        wide
        * lax.rsqrt(jnp.mean(wide * wide, axis=-1, keepdims=True) + epsilon)
        * gain_ref[...]
    ).astype(BF16)
    all_rows = (seqs * heads, seqs)
    repeat = (lax.shift_right_logical(iota(all_rows, 0), log2(heads)) == iota(all_rows, 1)).astype(
        F32
    )
    repeat_b = repeat.astype(BF16)
    copies[2].wait()
    forget_logit = lax.dot_general(normed, forget_ref[...], NT, preferred_element_type=F32)
    log_forget = jax.nn.log_sigmoid(forget_logit)
    spread = jnp.dot(repeat, log_forget, precision=lax.Precision.HIGHEST, preferred_element_type=F32)
    head_of_row = jnp.bitwise_and(iota(spread.shape, 0), heads - 1)
    forget_col[...] = jnp.sum(
        jnp.where(iota(spread.shape, 1) == head_of_row + head_start, spread, 0.0),
        axis=1,
        keepdims=True,
    )
    copies[3].wait()
    query = dot(normed, query_w[...]).astype(BF16)
    copies[4].wait()
    fresh_key = dot(normed, key_w[...]).astype(BF16)
    copies[5].wait()
    fresh_value = dot(normed, value_w[...]).astype(BF16)
    wide_shape = (seqs * heads, head_width)
    own_head = lax.shift_right_logical(iota(wide_shape, 1), log2(head_dim)) == jnp.bitwise_and(
        iota(wide_shape, 0), heads - 1
    )
    fold_shape = (head_width, kv_width)
    fold_row = iota(fold_shape, 0)
    fold = (
        iota(fold_shape, 1)
        == lax.shift_right_logical(fold_row, log2(heads // kv * head_dim)) * head_dim
        + jnp.bitwise_and(fold_row, head_dim - 1)
    ).astype(F32).astype(BF16)
    spread_query = jnp.where(own_head, dot(repeat_b, query), 0.0).astype(BF16)
    folded = dot(spread_query, fold)
    member = jnp.bitwise_and(
        lax.shift_right_logical(iota(folded.shape, 0), log2(heads)), group - 1
    )
    for m in range(group):
        wide_query[:, m * kv_width : (m + 1) * kv_width] = jnp.where(
            member == m, folded, 0.0
        ).astype(BF16)
    scale = head_dim ** (-0.5)
    new_col[...] = (
        jnp.sum(folded * dot(repeat_b, fresh_key), axis=1, keepdims=True) * scale
    )
    new_value[...] = dot(repeat_b, fresh_value)

    position = iota((rows, span), 1)
    row_member = lax.shift_right_logical(iota((rows, span), 0), log2(heads))
    small_member = lax.shift_right_logical(iota((rows, kv_width), 0), log2(heads))

    def scores(g):
        cache_copy(g, 0).wait()
        at = slice(g * rows, (g + 1) * rows)
        part = slice(g * group, (g + 1) * group)
        raw = dot(wide_query[at, :], keys[part].reshape(group * kv_width, span))
        cache_copy(g, 1).wait()
        gate = gates[part].reshape(rows, span)
        length = jnp.full((rows, span), lengths_ref[g * group], jnp.int32)
        for m in range(1, group):
            length = jnp.where(row_member == m, lengths_ref[g * group + m], length)
        latest = jnp.sum(
            jnp.where(position == length - 1, gate, 0.0), axis=1, keepdims=True
        )
        past = raw * scale + (latest + forget_col[at, :]) - gate
        past = jnp.where(position < length, past, -jnp.inf)
        fresh = new_col[at, :]
        peak = jnp.maximum(jnp.max(past, axis=1, keepdims=True), fresh)
        past_exp = jnp.exp(past - peak)
        new_exp = jnp.exp(fresh - peak)
        total = jnp.sum(past_exp, axis=1, keepdims=True) + new_exp
        return past_exp.astype(BF16), new_exp, total

    def mix(g, past_exp, new_exp, total):
        cache_copy(g, 2).wait()
        at = slice(g * rows, (g + 1) * rows)
        part = slice(g * group, (g + 1) * group)
        out = lax.dot_general(
            past_exp,
            values[part].reshape(group * kv_width, span),
            NT,
            preferred_element_type=F32,
        )
        own = jnp.zeros((rows, kv_width), F32)
        for m in range(group):
            own = jnp.where(small_member == m, out[:, m * kv_width : (m + 1) * kv_width], own)
        mixed[at, :] = ((own + new_exp * new_value[at, :]) / total).astype(BF16)

    ready = scores(0)
    for g in range(groups):
        after = scores(g + 1) if g + 1 < groups else None
        mix(g, *ready)
        ready = after

    unfolded = lax.dot_general(mixed[...], fold, NT, preferred_element_type=F32)
    unfolded = jnp.where(own_head, unfolded, 0.0).astype(BF16)
    gather_shape = (seqs, seqs * heads)
    gather = (
        lax.shift_right_logical(iota(gather_shape, 1), log2(heads)) == iota(gather_shape, 0)
    ).astype(F32).astype(BF16)
    attended = dot(gather, unfolded).astype(BF16)
    copies[-1].wait()
    own_width = keep_ref.shape[1] // y_count
    for y in range(y_count):
        at = slice(y * own_width, (y + 1) * own_width)
        for ref, which in ((send_ref, 1 - core), (keep_ref, core)):
            start = pl.multiple_of((y * CORES + which) * own_width, own_width)
            ref[:, at] = dot(attended, out_w[:, pl.ds(start, own_width)]).astype(ref.dtype)


def dispatch_kernel(
    y_count, where_ref, tokens_ref, mine_ref, theirs_ref, dispatch_ref, packed_ref, own_ref
):
    core = where_ref[0]
    y_index = where_ref[2]
    own_width = own_ref.shape[1]
    for y in range(y_count):
        at = slice(y * own_width, (y + 1) * own_width)
        start = pl.multiple_of((y * CORES + core) * own_width, own_width)
        attention = mine_ref[:, at] + theirs_ref[:, at].astype(F32)
        stream = tokens_ref[:, pl.ds(start, own_width)].astype(F32) + attention
        packed_ref[:, at] = dot(dispatch_ref[...], stream.astype(BF16)).astype(BF16)

        @pl.when(y_index == y)
        def _():
            own_ref[...] = stream


def expert_kernel(
    sizes,
    where_ref,
    mine_ref,
    theirs_ref,
    gain_ref,
    gate_w,
    up_w,
    down_w,
    keep_ref,
    send_ref,
):
    y_count, ep_count, capacity = sizes
    core = where_ref[0]
    half = mine_ref.shape[1]
    own_width = half // y_count
    rows = mine_ref.shape[0]
    width = half * CORES
    total = jnp.zeros((rows, 1), F32)
    for ref in (mine_ref, theirs_ref):
        x = ref[...].astype(F32)
        total = total + jnp.sum(x * x, axis=1, keepdims=True)
    inverse = lax.rsqrt(total / width + epsilon)
    gate_act = jnp.zeros((rows, gate_w.shape[2]), F32)
    upper = jnp.zeros((rows, gate_w.shape[2]), F32)
    for ref, which in ((mine_ref, core), (theirs_ref, 1 - core)):
        for y in range(y_count):
            start = pl.multiple_of((y * CORES + which) * own_width, own_width)
            x = ref[:, y * own_width : (y + 1) * own_width].astype(F32)
            x = (x * inverse * gain_ref[:, pl.ds(start, own_width)]).astype(BF16)
            gate_act = gate_act + dot(x, gate_w[0, pl.ds(start, own_width), :])
            upper = upper + dot(x, up_w[0, pl.ds(start, own_width), :])
    hidden = (gate_act / (1.0 + jnp.exp(-gate_act)) * upper).astype(BF16)
    for y in range(y_count):
        for ref, which in ((send_ref, 1 - core), (keep_ref, core)):
            start = pl.multiple_of((y * CORES + which) * own_width, own_width)
            part = dot(hidden, down_w[0, :, pl.ds(start, own_width)]).astype(ref.dtype)
            for e in range(ep_count):
                ref[e, y] = part[e * capacity : (e + 1) * capacity, :]


def combine_kernel(stream_ref, combine_ref, returned_ref, out_ref):
    weight = combine_ref[...]
    high = weight.astype(BF16)
    low = (weight - high.astype(F32)).astype(BF16)
    rows = returned_ref[...]
    out_ref[...] = (stream_ref[...] + (dot(high, rows) + dot(low, rows))).astype(out_ref.dtype)


def call(kernel, shapes, args, where, **params):
    specs = [pl.BlockSpec(memory_space=pltpu.SMEM)] * (1 if where is not None else 0)
    given = ((where,) if where is not None else ()) + tuple(args)
    specs += [pl.BlockSpec(memory_space=pltpu.VMEM)] * len(args)
    many = isinstance(shapes, (list, tuple))
    vmem = pl.BlockSpec(memory_space=pltpu.VMEM)
    return pl.pallas_call(
        kernel,
        out_shape=shapes,
        in_specs=specs,
        out_specs=[vmem] * len(shapes) if many else vmem,
        compiler_params=pltpu.CompilerParams(vmem_limit_bytes=40 * 1024 * 1024),
        **params,
    )(*given)


def body(
    tokens,
    norm_gain,
    post_gain,
    w_query,
    w_key,
    w_value,
    w_forget,
    w_output,
    key_cache,
    value_cache,
    gate_cache,
    lengths,
    routes,
    route_logits,
    w_gate,
    w_up,
    w_down,
):
    ep_count = lax.axis_size("ep")
    y_count = lax.axis_size("y")
    core = lax.axis_index("core")
    y_index = lax.axis_index("y")
    seqs, width = tokens.shape
    kv, head_dim, span = key_cache.shape[1:]
    heads = gate_cache.shape[1]
    own_width = width // (y_count * CORES)
    half = own_width * y_count
    capacity = 2 * seqs * routes.shape[1] // ep_count
    slot_count = ep_count * capacity
    group = min(seqs, max(1, 256 // (kv * head_dim)))
    where = jnp.stack([core, (y_index * CORES + core) * heads, y_index]).astype(jnp.int32)
    shape = jax.ShapeDtypeStruct
    sizes = (seqs, heads, kv, head_dim, span, group, y_count, ep_count, capacity)
    kv_width = kv * head_dim
    all_rows = seqs * heads
    smem = pl.BlockSpec(memory_space=pltpu.SMEM)
    vmem = pl.BlockSpec(memory_space=pltpu.VMEM)
    hbm = pl.BlockSpec(memory_space=pl.ANY)
    forget_t = w_forget.T
    keep, send, dispatch, combine = pl.pallas_call(
        functools.partial(attention_kernel, sizes),
        out_shape=[
            shape((seqs, half), F32),
            shape((seqs, half), BF16),
            shape((slot_count, seqs), BF16),
            shape((seqs, y_count * slot_count), F32),
        ],
        in_specs=[smem, smem] + [hbm] * 10 + [vmem, vmem],
        out_specs=[vmem] * 4,
        scratch_shapes=[
            pltpu.VMEM(tokens.shape, BF16),
            pltpu.VMEM((1, width), F32),
            pltpu.VMEM(forget_t.shape, BF16),
            pltpu.VMEM(w_query.shape, BF16),
            pltpu.VMEM(w_key.shape, BF16),
            pltpu.VMEM(w_value.shape, BF16),
            pltpu.VMEM(w_output.shape, BF16),
            pltpu.VMEM(key_cache.shape, BF16),
            pltpu.VMEM(value_cache.shape, BF16),
            pltpu.VMEM(gate_cache.shape, F32),
            pltpu.VMEM((all_rows, group * kv_width), BF16),
            pltpu.VMEM((all_rows, kv_width), BF16),
            pltpu.VMEM((all_rows, 1), F32),
            pltpu.VMEM((all_rows, 1), F32),
            pltpu.VMEM((all_rows, kv_width), F32),
            pltpu.SemaphoreType.DMA((7,)),
            pltpu.SemaphoreType.DMA((seqs // group, 3)),
        ],
        compiler_params=pltpu.CompilerParams(vmem_limit_bytes=40 * 1024 * 1024),
        name="attend",
    )(
        where,
        lengths,
        tokens,
        norm_gain.reshape(1, width),
        forget_t,
        w_query,
        w_key,
        w_value,
        w_output,
        key_cache,
        value_cache,
        gate_cache,
        routes.T,
        route_logits.T,
    )
    swap = [(i, 1 - i) for i in range(CORES)]
    mine = keep + lax.ppermute(send, "core", swap).astype(F32)
    if y_count == 2:
        theirs = lax.ppermute(mine.astype(BF16), "y", [(0, 1), (1, 0)])
    else:
        parts = lax.all_gather(mine.astype(BF16), "y")
        theirs = jnp.sum(parts.astype(F32), axis=0)
        mine = jnp.zeros_like(mine)
    packed, stream = call(
        functools.partial(dispatch_kernel, y_count),
        [shape((slot_count, half), BF16), shape((seqs, own_width), F32)],
        (tokens, mine, theirs, dispatch),
        where,
        name="dispatch",
    )
    arrived = lax.all_to_all(
        packed.reshape(ep_count, capacity, half), "ep", split_axis=0, concat_axis=0, tiled=True
    ).reshape(slot_count, half)
    beside = lax.ppermute(arrived, "core", swap)
    back = (ep_count, y_count, capacity, own_width)
    keep, send = call(
        functools.partial(expert_kernel, (y_count, ep_count, capacity)),
        [shape(back, F32), shape(back, BF16)],
        (arrived, beside, post_gain.reshape(1, width), w_gate, w_up, w_down),
        where,
        name="experts",
    )
    summed = (keep + lax.ppermute(send, "core", swap).astype(F32)).astype(BF16)
    returned = lax.all_to_all(
        summed.reshape(ep_count * y_count, capacity, own_width),
        ("ep", "y"),
        split_axis=0,
        concat_axis=0,
        tiled=True,
    ).reshape(ep_count * y_count * capacity, own_width)
    return call(
        combine_kernel,
        shape((seqs, own_width), BF16),
        (stream, combine, returned),
        None,
        name="combine",
    )


def solution(mesh):
    ep_count, tp_count = mesh.devices.shape
    inner = Mesh(
        mesh.devices.reshape(ep_count, tp_count // CORES, CORES), ("ep", "y", "core")
    )
    tp = ("y", "core")
    in_specs = (
        P("ep", None),
        P(),
        P(),
        P(None, tp),
        P(None, tp),
        P(None, tp),
        P(),
        P(tp, None),
        P("ep", tp, None, None),
        P("ep", tp, None, None),
        P("ep", tp, None),
        P("ep"),
        P("ep", None),
        P("ep", None),
        P("ep", None, tp),
        P("ep", None, tp),
        P("ep", tp, None),
    )
    return jax.shard_map(
        body, mesh=inner, in_specs=in_specs, out_specs=P("ep", tp), check_vma=False
    )
```

```python
import functools

import jax
import jax.numpy as jnp
from jax import lax
from jax.experimental import pallas as pl
from jax.experimental.pallas import tpu as pltpu
from jax.sharding import Mesh
from jax.sharding import PartitionSpec as P

epsilon = 1e-06
CORES = 2
CHUNKS = 4
AHEAD = 3
F32 = jnp.float32
BF16 = jnp.bfloat16
NT = (((1,), (1,)), ((), ()))


def log2(n):
    assert n & (n - 1) == 0
    return n.bit_length() - 1


def dot(a, b):
    return jnp.dot(a, b, preferred_element_type=F32)


def iota(shape, axis):
    return lax.broadcasted_iota(jnp.int32, shape, axis)


def attention_kernel(
    sizes,
    lengths_hbm,
    tokens_hbm,
    gain_hbm,
    forget_hbm,
    query_hbm,
    key_w_hbm,
    value_w_hbm,
    out_w_hbm,
    key_hbm,
    value_hbm,
    gate_hbm,
    routes_hbm,
    logits_hbm,
    keep_ref,
    send_ref,
    dispatch_ref,
    combine_ref,
    lengths_ref,
    routes_ref,
    logits_ref,
    tokens_ref,
    gain_ref,
    forget_ref,
    query_w,
    key_w,
    value_w,
    out_w,
    keys,
    values,
    gates,
    wide_query,
    mixed,
    forget_col,
    new_col,
    new_value,
    probs,
    new_exps,
    totals,
    first_sems,
    cache_sems,
):
    seqs, heads, kv, head_dim, span, group, y_count, ep_count, capacity = sizes
    groups = seqs // group
    rows = group * heads
    kv_width = kv * head_dim
    head_width = heads * head_dim
    firsts = [
        (tokens_hbm, tokens_ref),
        (gain_hbm, gain_ref),
        (forget_hbm, forget_ref),
        (query_hbm, query_w),
        (key_w_hbm, key_w),
        (value_w_hbm, value_w),
        (lengths_hbm, lengths_ref),
        (routes_hbm, routes_ref),
        (logits_hbm, logits_ref),
        (out_w_hbm, out_w),
    ]
    copies = [
        pltpu.make_async_copy(src, dst, first_sems.at[i]) for i, (src, dst) in enumerate(firsts)
    ]

    caches = ((key_hbm, keys), (gate_hbm, gates), (value_hbm, values))

    chunks = cache_sems.shape[0]
    chunk = groups // chunks

    def cache_copy(c, i):
        part = pl.ds(c * chunk * group, chunk * group)
        src, dst = caches[i]
        return pltpu.make_async_copy(src.at[part], dst.at[part], cache_sems.at[c, i])

    def start_chunk(c):
        if c < chunks:
            for i in range(3):
                cache_copy(c, i).start()
        elif c == chunks:
            copies[-1].start()

    for c in copies[:-1]:
        c.start()
    start_chunk(0)

    core = lax.axis_index("core")
    head_start = (lax.axis_index("y") * CORES + core) * heads

    for c in copies[:-1]:
        c.wait()
    for c in range(1, AHEAD):
        start_chunk(c)

    experts = iota((ep_count, seqs), 0)
    picks = [routes_ref[k : k + 1, :] for k in range(2)]
    named = jnp.zeros((ep_count, seqs), F32)
    for k in range(2):
        named = named + (experts == picks[k]).astype(F32)
    earlier = (iota((seqs, seqs), 0) < iota((seqs, seqs), 1)).astype(BF16)
    rank = dot(named.astype(BF16), earlier)
    slot_of = experts.astype(F32) * capacity + rank
    slots = [
        jnp.sum(jnp.where(experts == picks[k], slot_of, 0.0), axis=0, keepdims=True)
        for k in range(2)
    ]
    slot_iota = iota((ep_count * capacity, seqs), 0).astype(F32)
    dispatch_ref[...] = jnp.logical_or(slot_iota == slots[0], slot_iota == slots[1]).astype(
        F32
    ).astype(BF16)
    logits = [logits_ref[k : k + 1, :] for k in range(2)]
    top = jnp.maximum(logits[0], logits[1])
    raised = [jnp.exp(x - top) for x in logits]
    total = raised[0] + raised[1]
    eye = iota((seqs, seqs), 0) == iota((seqs, seqs), 1)

    def column(x):
        return jnp.sum(jnp.where(eye, x, 0.0), axis=1, keepdims=True)

    returned = (seqs, ep_count * y_count * capacity)
    back = iota(returned, 1)
    back_slot = (
        lax.shift_right_logical(back, log2(y_count * capacity)) * capacity
        + jnp.bitwise_and(back, capacity - 1)
    ).astype(F32)
    combine_ref[...] = jnp.where(
        back_slot == column(slots[0]), column(raised[0] / total), 0.0
    ) + jnp.where(back_slot == column(slots[1]), column(raised[1] / total), 0.0)

    wide = tokens_ref[...].astype(F32)
    normed = (
        wide
        * lax.rsqrt(jnp.mean(wide * wide, axis=-1, keepdims=True) + epsilon)
        * gain_ref[...]
    ).astype(BF16)
    all_rows = (seqs * heads, seqs)
    repeat = (lax.shift_right_logical(iota(all_rows, 0), log2(heads)) == iota(all_rows, 1)).astype(
        F32
    )
    repeat_b = repeat.astype(BF16)
    forget_logit = lax.dot_general(normed, forget_ref[...], NT, preferred_element_type=F32)
    log_forget = jax.nn.log_sigmoid(forget_logit)
    spread = jnp.dot(repeat, log_forget, precision=lax.Precision.HIGHEST, preferred_element_type=F32)
    head_of_row = jnp.bitwise_and(iota(spread.shape, 0), heads - 1)
    forget_col[...] = jnp.sum(
        jnp.where(iota(spread.shape, 1) == head_of_row + head_start, spread, 0.0),
        axis=1,
        keepdims=True,
    )
    query = dot(normed, query_w[...]).astype(BF16)
    fresh_key = dot(normed, key_w[...]).astype(BF16)
    fresh_value = dot(normed, value_w[...]).astype(BF16)
    wide_shape = (seqs * heads, head_width)
    own_head = lax.shift_right_logical(iota(wide_shape, 1), log2(head_dim)) == jnp.bitwise_and(
        iota(wide_shape, 0), heads - 1
    )
    fold_shape = (head_width, kv_width)
    fold_row = iota(fold_shape, 0)
    fold = (
        iota(fold_shape, 1)
        == lax.shift_right_logical(fold_row, log2(heads // kv * head_dim)) * head_dim
        + jnp.bitwise_and(fold_row, head_dim - 1)
    ).astype(F32).astype(BF16)
    spread_query = jnp.where(own_head, dot(repeat_b, query), 0.0).astype(BF16)
    folded = dot(spread_query, fold)
    member = jnp.bitwise_and(
        lax.shift_right_logical(iota(folded.shape, 0), log2(heads)), group - 1
    )
    for m in range(group):
        wide_query[:, m * kv_width : (m + 1) * kv_width] = jnp.where(
            member == m, folded, 0.0
        ).astype(BF16)
    scale = head_dim ** (-0.5)
    new_col[...] = (
        jnp.sum(folded * dot(repeat_b, fresh_key), axis=1, keepdims=True) * scale
    )
    new_value[...] = dot(repeat_b, fresh_value)

    position = iota((rows, span), 1)
    row_member = lax.shift_right_logical(iota((rows, span), 0), log2(heads))
    small_member = lax.shift_right_logical(iota((rows, kv_width), 0), log2(heads))

    def scores(g):
        at = slice(g * rows, (g + 1) * rows)
        part = slice(g * group, (g + 1) * group)
        raw = dot(wide_query[at, :], keys[part].reshape(group * kv_width, span))
        gate = gates[part].reshape(rows, span)
        length = jnp.full((rows, span), lengths_ref[g * group], jnp.int32)
        for m in range(1, group):
            length = jnp.where(row_member == m, lengths_ref[g * group + m], length)
        latest = jnp.sum(
            jnp.where(position == length - 1, gate, 0.0), axis=1, keepdims=True
        )
        past = raw * scale + (latest + forget_col[at, :]) - gate
        past = jnp.where(position < length, past, -jnp.inf)
        fresh = new_col[at, :]
        peak = jnp.maximum(jnp.max(past, axis=1, keepdims=True), fresh)
        past_exp = jnp.exp(past - peak)
        new_exp = jnp.exp(fresh - peak)
        total = jnp.sum(past_exp, axis=1, keepdims=True) + new_exp
        probs[at, :] = past_exp.astype(BF16)
        new_exps[at, :] = new_exp
        totals[at, :] = total

    def mix(g):
        at = slice(g * rows, (g + 1) * rows)
        part = slice(g * group, (g + 1) * group)
        out = lax.dot_general(
            probs[at, :],
            values[part].reshape(group * kv_width, span),
            NT,
            preferred_element_type=F32,
        )
        own = jnp.zeros((rows, kv_width), F32)
        for m in range(group):
            own = jnp.where(small_member == m, out[:, m * kv_width : (m + 1) * kv_width], own)
        mixed[at, :] = ((own + new_exps[at, :] * new_value[at, :]) / totals[at, :]).astype(BF16)

    for c in range(chunks + 1):
        if c < chunks:
            cache_copy(c, 0).wait()
            cache_copy(c, 1).wait()
        if c > 0:
            cache_copy(c - 1, 2).wait()
        start_chunk(c + AHEAD)
        for j in range(chunk):
            if c < chunks:
                scores(c * chunk + j)
            if c > 0:
                mix((c - 1) * chunk + j)

    unfolded = lax.dot_general(mixed[...], fold, NT, preferred_element_type=F32)
    unfolded = jnp.where(own_head, unfolded, 0.0).astype(BF16)
    gather_shape = (seqs, seqs * heads)
    gather = (
        lax.shift_right_logical(iota(gather_shape, 1), log2(heads)) == iota(gather_shape, 0)
    ).astype(F32).astype(BF16)
    attended = dot(gather, unfolded).astype(BF16)
    copies[-1].wait()
    own_width = keep_ref.shape[1] // y_count
    for y in range(y_count):
        at = slice(y * own_width, (y + 1) * own_width)
        for ref, which in ((send_ref, 1 - core), (keep_ref, core)):
            start = pl.multiple_of((y * CORES + which) * own_width, own_width)
            ref[:, at] = dot(attended, out_w[:, pl.ds(start, own_width)]).astype(ref.dtype)


def dispatch_kernel(
    y_count, tokens_ref, mine_ref, theirs_ref, dispatch_ref, packed_ref, own_ref
):
    core = lax.axis_index("core")
    y_index = lax.axis_index("y")
    own_width = own_ref.shape[1]
    for y in range(y_count):
        at = slice(y * own_width, (y + 1) * own_width)
        start = pl.multiple_of((y * CORES + core) * own_width, own_width)
        attention = mine_ref[:, at] + theirs_ref[:, at].astype(F32)
        stream = tokens_ref[:, pl.ds(start, own_width)].astype(F32) + attention
        packed_ref[:, at] = dot(dispatch_ref[...], stream.astype(BF16)).astype(BF16)

        @pl.when(y_index == y)
        def _():
            own_ref[...] = stream


def expert_kernel(
    sizes,
    mine_ref,
    theirs_ref,
    gain_ref,
    gate_w,
    up_w,
    down_w,
    keep_ref,
    send_ref,
):
    y_count, ep_count, capacity = sizes
    core = lax.axis_index("core")
    half = mine_ref.shape[1]
    own_width = half // y_count
    rows = mine_ref.shape[0]
    width = half * CORES
    total = jnp.zeros((rows, 1), F32)
    for ref in (mine_ref, theirs_ref):
        x = ref[...].astype(F32)
        total = total + jnp.sum(x * x, axis=1, keepdims=True)
    inverse = lax.rsqrt(total / width + epsilon)
    gate_act = jnp.zeros((rows, gate_w.shape[2]), F32)
    upper = jnp.zeros((rows, gate_w.shape[2]), F32)
    for ref, which in ((mine_ref, core), (theirs_ref, 1 - core)):
        for y in range(y_count):
            start = pl.multiple_of((y * CORES + which) * own_width, own_width)
            x = ref[:, y * own_width : (y + 1) * own_width].astype(F32)
            x = (x * inverse * gain_ref[:, pl.ds(start, own_width)]).astype(BF16)
            gate_act = gate_act + dot(x, gate_w[0, pl.ds(start, own_width), :])
            upper = upper + dot(x, up_w[0, pl.ds(start, own_width), :])
    hidden = (gate_act / (1.0 + jnp.exp(-gate_act)) * upper).astype(BF16)
    for y in range(y_count):
        for ref, which in ((send_ref, 1 - core), (keep_ref, core)):
            start = pl.multiple_of((y * CORES + which) * own_width, own_width)
            part = dot(hidden, down_w[0, :, pl.ds(start, own_width)]).astype(ref.dtype)
            for e in range(ep_count):
                ref[e, y] = part[e * capacity : (e + 1) * capacity, :]


def combine_kernel(stream_ref, combine_ref, returned_ref, out_ref):
    weight = combine_ref[...]
    high = weight.astype(BF16)
    low = (weight - high.astype(F32)).astype(BF16)
    rows = returned_ref[...]
    out_ref[...] = (stream_ref[...] + (dot(high, rows) + dot(low, rows))).astype(out_ref.dtype)


def call(kernel, shapes, args, **params):
    vmem = pl.BlockSpec(memory_space=pltpu.VMEM)
    many = isinstance(shapes, (list, tuple))
    return pl.pallas_call(
        kernel,
        out_shape=shapes,
        in_specs=[vmem] * len(args),
        out_specs=[vmem] * len(shapes) if many else vmem,
        compiler_params=pltpu.CompilerParams(vmem_limit_bytes=40 * 1024 * 1024),
        **params,
    )(*args)


def attend(
    lengths,
    tokens,
    norm_gain,
    w_forget,
    w_query,
    w_key,
    w_value,
    w_output,
    key_cache,
    value_cache,
    gate_cache,
    routes,
    route_logits,
    y_count,
    ep_count,
):
    seqs, width = tokens.shape
    kv, head_dim, span = key_cache.shape[1:]
    heads = gate_cache.shape[1]
    half = width // CORES
    capacity = 2 * seqs * routes.shape[1] // ep_count
    slot_count = ep_count * capacity
    group = min(seqs, max(1, 256 // (kv * head_dim)))
    sizes = (seqs, heads, kv, head_dim, span, group, y_count, ep_count, capacity)
    kv_width = kv * head_dim
    all_rows = seqs * heads
    shape = jax.ShapeDtypeStruct
    vmem = pl.BlockSpec(memory_space=pltpu.VMEM)
    hbm = pl.BlockSpec(memory_space=pltpu.HBM)
    forget_t = w_forget.T
    routes_t = routes.T
    return pl.pallas_call(
        functools.partial(attention_kernel, sizes),
        out_shape=[
            shape((seqs, half), F32),
            shape((seqs, half), BF16),
            shape((slot_count, seqs), BF16),
            shape((seqs, y_count * slot_count), F32),
        ],
        in_specs=[hbm] * 13,
        out_specs=[vmem] * 4,
        scratch_shapes=[
            pltpu.SMEM(lengths.shape, jnp.int32),
            pltpu.VMEM(routes_t.shape, jnp.int32),
            pltpu.VMEM(routes_t.shape, F32),
            pltpu.VMEM(tokens.shape, BF16),
            pltpu.VMEM((1, width), F32),
            pltpu.VMEM(forget_t.shape, BF16),
            pltpu.VMEM(w_query.shape, BF16),
            pltpu.VMEM(w_key.shape, BF16),
            pltpu.VMEM(w_value.shape, BF16),
            pltpu.VMEM(w_output.shape, BF16),
            pltpu.VMEM(key_cache.shape, BF16),
            pltpu.VMEM(value_cache.shape, BF16),
            pltpu.VMEM(gate_cache.shape, F32),
            pltpu.VMEM((all_rows, group * kv_width), BF16),
            pltpu.VMEM((all_rows, kv_width), BF16),
            pltpu.VMEM((all_rows, 1), F32),
            pltpu.VMEM((all_rows, 1), F32),
            pltpu.VMEM((all_rows, kv_width), F32),
            pltpu.VMEM((all_rows, span), BF16),
            pltpu.VMEM((all_rows, 1), F32),
            pltpu.VMEM((all_rows, 1), F32),
            pltpu.SemaphoreType.DMA((10,)),
            pltpu.SemaphoreType.DMA((min(CHUNKS, seqs // group), 3)),
        ],
        compiler_params=pltpu.CompilerParams(vmem_limit_bytes=40 * 1024 * 1024),
        name="attend",
    )(
        *[
            pltpu.with_memory_space_constraint(x, pltpu.HBM)
            for x in (
                lengths,
                tokens,
                norm_gain.reshape(1, width),
                forget_t,
                w_query,
                w_key,
                w_value,
                w_output,
                key_cache,
                value_cache,
                gate_cache,
                routes_t,
                route_logits.T,
            )
        ]
    )


def body(
    tokens,
    norm_gain,
    post_gain,
    w_query,
    w_key,
    w_value,
    w_forget,
    w_output,
    key_cache,
    value_cache,
    gate_cache,
    lengths,
    routes,
    route_logits,
    w_gate,
    w_up,
    w_down,
):
    ep_count = lax.axis_size("ep")
    y_count = lax.axis_size("y")
    seqs, width = tokens.shape
    heads = gate_cache.shape[1]
    own_width = width // (y_count * CORES)
    half = own_width * y_count
    capacity = 2 * seqs * routes.shape[1] // ep_count
    slot_count = ep_count * capacity
    shape = jax.ShapeDtypeStruct
    keep, send, dispatch, combine = attend(
        lengths,
        tokens,
        norm_gain,
        w_forget,
        w_query,
        w_key,
        w_value,
        w_output,
        key_cache,
        value_cache,
        gate_cache,
        routes,
        route_logits,
        y_count,
        ep_count,
    )
    send, w_gate, w_up, w_down = lax.optimization_barrier((send, w_gate, w_up, w_down))
    swap = [(i, 1 - i) for i in range(CORES)]
    mine = keep + lax.ppermute(send, "core", swap).astype(F32)
    if y_count == 2:
        theirs = lax.ppermute(mine.astype(BF16), "y", [(0, 1), (1, 0)])
    else:
        parts = lax.all_gather(mine.astype(BF16), "y")
        theirs = jnp.sum(parts.astype(F32), axis=0)
        mine = jnp.zeros_like(mine)
    packed, stream = call(
        functools.partial(dispatch_kernel, y_count),
        [shape((slot_count, half), BF16), shape((seqs, own_width), F32)],
        (tokens, mine, theirs, dispatch),
        name="dispatch",
    )
    arrived = lax.all_to_all(
        packed.reshape(ep_count, capacity, half), "ep", split_axis=0, concat_axis=0, tiled=True
    ).reshape(slot_count, half)
    beside = lax.ppermute(arrived, "core", swap)
    back = (ep_count, y_count, capacity, own_width)
    keep, send = call(
        functools.partial(expert_kernel, (y_count, ep_count, capacity)),
        [shape(back, F32), shape(back, BF16)],
        (arrived, beside, post_gain.reshape(1, width), w_gate, w_up, w_down),
        name="experts",
    )
    summed = (keep + lax.ppermute(send, "core", swap).astype(F32)).astype(BF16)
    returned = lax.all_to_all(
        summed.reshape(ep_count * y_count, capacity, own_width),
        ("ep", "y"),
        split_axis=0,
        concat_axis=0,
        tiled=True,
    ).reshape(ep_count * y_count * capacity, own_width)
    return call(
        combine_kernel,
        shape((seqs, own_width), BF16),
        (stream, combine, returned),
        name="combine",
    )


def solution(mesh):
    ep_count, tp_count = mesh.devices.shape
    inner = Mesh(
        mesh.devices.reshape(ep_count, tp_count // CORES, CORES), ("ep", "y", "core")
    )
    tp = ("y", "core")
    in_specs = (
        P("ep", None),
        P(),
        P(),
        P(None, tp),
        P(None, tp),
        P(None, tp),
        P(),
        P(tp, None),
        P("ep", tp, None, None),
        P("ep", tp, None, None),
        P("ep", tp, None),
        P("ep"),
        P("ep", None),
        P("ep", None),
        P("ep", None, tp),
        P("ep", None, tp),
        P("ep", tp, None),
    )
    return jax.shard_map(
        body, mesh=inner, in_specs=in_specs, out_specs=P("ep", tp), check_vma=False
    )
```

```python
import functools
import itertools

import jax
import jax.numpy as jnp
from jax import lax
from jax.experimental import pallas as pl
from jax.experimental.pallas import tpu as pltpu
from jax.sharding import Mesh
from jax.sharding import PartitionSpec as P

epsilon = 1e-06
CORES = 2
SHARES = (0, 5, 9, 12, 14, 16)
AHEAD = 3
PREFETCH_HINT = 10**11
F32 = jnp.float32
BF16 = jnp.bfloat16
NT = (((1,), (1,)), ((), ()))


def log2(n):
    assert n & (n - 1) == 0
    return n.bit_length() - 1


def dot(a, b):
    return jnp.dot(a, b, preferred_element_type=F32)


def iota(shape, axis):
    return lax.broadcasted_iota(jnp.int32, shape, axis)


def attention_kernel(
    sizes,
    lengths_hbm,
    tokens_hbm,
    gain_hbm,
    forget_hbm,
    query_hbm,
    key_w_hbm,
    value_w_hbm,
    out_w_hbm,
    key_hbm,
    value_hbm,
    gate_hbm,
    routes_hbm,
    logits_hbm,
    keep_ref,
    send_ref,
    dispatch_ref,
    combine_ref,
    lengths_ref,
    routes_ref,
    logits_ref,
    tokens_ref,
    gain_ref,
    forget_ref,
    query_w,
    key_w,
    value_w,
    out_w,
    keys,
    values,
    gates,
    wide_query,
    mixed,
    forget_col,
    new_col,
    new_value,
    probs,
    new_exps,
    totals,
    first_sems,
    cache_sems,
):
    seqs, heads, kv, head_dim, span, group, bounds, y_count, ep_count, capacity = sizes
    groups = seqs // group
    rows = group * heads
    kv_width = kv * head_dim
    head_width = heads * head_dim
    firsts = [
        (tokens_hbm, tokens_ref),
        (gain_hbm, gain_ref),
        (forget_hbm, forget_ref),
        (query_hbm, query_w),
        (key_w_hbm, key_w),
        (value_w_hbm, value_w),
        (lengths_hbm, lengths_ref),
        (routes_hbm, routes_ref),
        (logits_hbm, logits_ref),
        (out_w_hbm, out_w),
    ]
    copies = [
        pltpu.make_async_copy(src, dst, first_sems.at[i]) for i, (src, dst) in enumerate(firsts)
    ]

    caches = ((key_hbm, keys), (gate_hbm, gates), (value_hbm, values))

    chunks = len(bounds) - 1

    def cache_copy(c, i):
        part = pl.ds(bounds[c] * group, (bounds[c + 1] - bounds[c]) * group)
        src, dst = caches[i]
        return pltpu.make_async_copy(src.at[part], dst.at[part], cache_sems.at[c, i])

    def start_chunk(c):
        if c < chunks:
            for i in range(3):
                cache_copy(c, i).start()
        elif c == chunks:
            copies[-1].start()

    for c in copies[:-1]:
        c.start()
    start_chunk(0)

    core = lax.axis_index("core")
    head_start = (lax.axis_index("y") * CORES + core) * heads

    for c in copies[:-1]:
        c.wait()
    for c in range(1, AHEAD):
        start_chunk(c)

    experts = iota((ep_count, seqs), 0)
    picks = [routes_ref[k : k + 1, :] for k in range(2)]
    named = jnp.zeros((ep_count, seqs), F32)
    for k in range(2):
        named = named + (experts == picks[k]).astype(F32)
    earlier = (iota((seqs, seqs), 0) < iota((seqs, seqs), 1)).astype(BF16)
    rank = dot(named.astype(BF16), earlier)
    slot_of = experts.astype(F32) * capacity + rank
    slots = [
        jnp.sum(jnp.where(experts == picks[k], slot_of, 0.0), axis=0, keepdims=True)
        for k in range(2)
    ]
    slot_iota = iota((ep_count * capacity, seqs), 0).astype(F32)
    dispatch_ref[...] = jnp.logical_or(slot_iota == slots[0], slot_iota == slots[1]).astype(
        F32
    ).astype(BF16)
    logits = [logits_ref[k : k + 1, :] for k in range(2)]
    top = jnp.maximum(logits[0], logits[1])
    raised = [jnp.exp(x - top) for x in logits]
    total = raised[0] + raised[1]
    eye = iota((seqs, seqs), 0) == iota((seqs, seqs), 1)

    def column(x):
        return jnp.sum(jnp.where(eye, x, 0.0), axis=1, keepdims=True)

    returned = (seqs, ep_count * y_count * capacity)
    back = iota(returned, 1)
    back_slot = (
        lax.shift_right_logical(back, log2(y_count * capacity)) * capacity
        + jnp.bitwise_and(back, capacity - 1)
    ).astype(F32)
    combine_ref[...] = jnp.where(
        back_slot == column(slots[0]), column(raised[0] / total), 0.0
    ) + jnp.where(back_slot == column(slots[1]), column(raised[1] / total), 0.0)

    wide = tokens_ref[...].astype(F32)
    normed = (
        wide
        * lax.rsqrt(jnp.mean(wide * wide, axis=-1, keepdims=True) + epsilon)
        * gain_ref[...]
    ).astype(BF16)
    all_rows = (seqs * heads, seqs)
    repeat = (lax.shift_right_logical(iota(all_rows, 0), log2(heads)) == iota(all_rows, 1)).astype(
        F32
    )
    repeat_b = repeat.astype(BF16)
    forget_logit = lax.dot_general(normed, forget_ref[...], NT, preferred_element_type=F32)
    log_forget = jax.nn.log_sigmoid(forget_logit)
    spread = jnp.dot(repeat, log_forget, precision=lax.Precision.HIGHEST, preferred_element_type=F32)
    head_of_row = jnp.bitwise_and(iota(spread.shape, 0), heads - 1)
    forget_col[...] = jnp.sum(
        jnp.where(iota(spread.shape, 1) == head_of_row + head_start, spread, 0.0),
        axis=1,
        keepdims=True,
    )
    query = dot(normed, query_w[...]).astype(BF16)
    fresh_key = dot(normed, key_w[...]).astype(BF16)
    fresh_value = dot(normed, value_w[...]).astype(BF16)
    wide_shape = (seqs * heads, head_width)
    own_head = lax.shift_right_logical(iota(wide_shape, 1), log2(head_dim)) == jnp.bitwise_and(
        iota(wide_shape, 0), heads - 1
    )
    fold_shape = (head_width, kv_width)
    fold_row = iota(fold_shape, 0)
    fold = (
        iota(fold_shape, 1)
        == lax.shift_right_logical(fold_row, log2(heads // kv * head_dim)) * head_dim
        + jnp.bitwise_and(fold_row, head_dim - 1)
    ).astype(F32).astype(BF16)
    spread_query = jnp.where(own_head, dot(repeat_b, query), 0.0).astype(BF16)
    folded = dot(spread_query, fold)
    member = jnp.bitwise_and(
        lax.shift_right_logical(iota(folded.shape, 0), log2(heads)), group - 1
    )
    for m in range(group):
        wide_query[:, m * kv_width : (m + 1) * kv_width] = jnp.where(
            member == m, folded, 0.0
        ).astype(BF16)
    scale = head_dim ** (-0.5)
    new_col[...] = (
        jnp.sum(folded * dot(repeat_b, fresh_key), axis=1, keepdims=True) * scale
    )
    new_value[...] = dot(repeat_b, fresh_value)

    position = iota((rows, span), 1)
    row_member = lax.shift_right_logical(iota((rows, span), 0), log2(heads))
    small_member = lax.shift_right_logical(iota((rows, kv_width), 0), log2(heads))

    def scores(g):
        at = slice(g * rows, (g + 1) * rows)
        part = slice(g * group, (g + 1) * group)
        raw = dot(wide_query[at, :], keys[part].reshape(group * kv_width, span))
        gate = gates[part].reshape(rows, span)
        length = jnp.full((rows, span), lengths_ref[g * group], jnp.int32)
        for m in range(1, group):
            length = jnp.where(row_member == m, lengths_ref[g * group + m], length)
        latest = jnp.sum(
            jnp.where(position == length - 1, gate, 0.0), axis=1, keepdims=True
        )
        past = raw * scale + (latest + forget_col[at, :]) - gate
        past = jnp.where(position < length, past, -jnp.inf)
        fresh = new_col[at, :]
        peak = jnp.maximum(jnp.max(past, axis=1, keepdims=True), fresh)
        past_exp = jnp.exp(past - peak)
        new_exp = jnp.exp(fresh - peak)
        total = jnp.sum(past_exp, axis=1, keepdims=True) + new_exp
        probs[at, :] = past_exp.astype(BF16)
        new_exps[at, :] = new_exp
        totals[at, :] = total

    def mix(g):
        at = slice(g * rows, (g + 1) * rows)
        part = slice(g * group, (g + 1) * group)
        out = lax.dot_general(
            probs[at, :],
            values[part].reshape(group * kv_width, span),
            NT,
            preferred_element_type=F32,
        )
        own = jnp.zeros((rows, kv_width), F32)
        for m in range(group):
            own = jnp.where(small_member == m, out[:, m * kv_width : (m + 1) * kv_width], own)
        mixed[at, :] = ((own + new_exps[at, :] * new_value[at, :]) / totals[at, :]).astype(BF16)

    for c in range(chunks + 1):
        if c < chunks:
            cache_copy(c, 0).wait()
            cache_copy(c, 1).wait()
        if c > 0:
            cache_copy(c - 1, 2).wait()
        start_chunk(c + AHEAD)
        new = range(bounds[c], bounds[c + 1]) if c < chunks else ()
        old = range(bounds[c - 1], bounds[c]) if c > 0 else ()
        for g, h in itertools.zip_longest(new, old):
            if g is not None:
                scores(g)
            if h is not None:
                mix(h)

    unfolded = lax.dot_general(mixed[...], fold, NT, preferred_element_type=F32)
    unfolded = jnp.where(own_head, unfolded, 0.0).astype(BF16)
    gather_shape = (seqs, seqs * heads)
    gather = (
        lax.shift_right_logical(iota(gather_shape, 1), log2(heads)) == iota(gather_shape, 0)
    ).astype(F32).astype(BF16)
    attended = dot(gather, unfolded).astype(BF16)
    copies[-1].wait()
    own_width = keep_ref.shape[1] // y_count
    for y in range(y_count):
        at = slice(y * own_width, (y + 1) * own_width)
        for ref, which in ((send_ref, 1 - core), (keep_ref, core)):
            start = pl.multiple_of((y * CORES + which) * own_width, own_width)
            ref[:, at] = dot(attended, out_w[:, pl.ds(start, own_width)]).astype(ref.dtype)


def dispatch_kernel(
    y_count, tokens_ref, mine_ref, theirs_ref, dispatch_ref, packed_ref, own_ref
):
    core = lax.axis_index("core")
    y_index = lax.axis_index("y")
    own_width = own_ref.shape[1]
    for y in range(y_count):
        at = slice(y * own_width, (y + 1) * own_width)
        start = pl.multiple_of((y * CORES + core) * own_width, own_width)
        attention = mine_ref[:, at] + theirs_ref[:, at].astype(F32)
        stream = tokens_ref[:, pl.ds(start, own_width)].astype(F32) + attention
        packed_ref[:, at] = dot(dispatch_ref[...], stream.astype(BF16)).astype(BF16)

        @pl.when(y_index == y)
        def _():
            own_ref[...] = stream


def half_products(rows_ref, which, y_count, gain_ref, gate_w, up_w):
    own_width = rows_ref.shape[1] // y_count
    squares, gate_act, upper = 0.0, 0.0, 0.0
    for y in range(y_count):
        start = pl.multiple_of((y * CORES + which) * own_width, own_width)
        part = pl.ds(start, own_width)
        x = rows_ref[:, y * own_width : (y + 1) * own_width].astype(F32)
        squares = squares + jnp.sum(x * x, axis=1, keepdims=True)
        x = (x * gain_ref[:, part]).astype(BF16)
        gate_act = gate_act + dot(x, gate_w[0, part, :])
        upper = upper + dot(x, up_w[0, part, :])
    return squares, gate_act, upper


def first_half_kernel(
    y_count, mine_ref, gain_ref, gate_w, up_w, down_w, squares_ref, gate_ref, upper_ref
):
    del down_w
    squares_ref[...], gate_ref[...], upper_ref[...] = half_products(
        mine_ref, lax.axis_index("core"), y_count, gain_ref, gate_w, up_w
    )


def down_half(hidden, which, down_w, ref):
    ep_count, y_count, capacity, own_width = ref.shape
    for y in range(y_count):
        start = pl.multiple_of((y * CORES + which) * own_width, own_width)
        part = dot(hidden, down_w[0, :, pl.ds(start, own_width)]).astype(ref.dtype)
        for e in range(ep_count):
            ref[e, y] = part[e * capacity : (e + 1) * capacity, :]


def second_half_kernel(
    theirs_ref,
    squares_ref,
    gate_ref,
    upper_ref,
    gain_ref,
    gate_w,
    up_w,
    down_w,
    hidden_ref,
    send_ref,
):
    other = 1 - lax.axis_index("core")
    y_count = send_ref.shape[1]
    width = theirs_ref.shape[1] * CORES
    squares, gate_act, upper = half_products(
        theirs_ref, other, y_count, gain_ref, gate_w, up_w
    )
    inverse = lax.rsqrt((squares + squares_ref[...]) / width + epsilon)
    gate_act = (gate_act + gate_ref[...]) * inverse
    upper = (upper + upper_ref[...]) * inverse
    hidden = (gate_act / (1.0 + jnp.exp(-gate_act)) * upper).astype(BF16)
    hidden_ref[...] = hidden
    down_half(hidden, other, down_w, send_ref)


def keep_kernel(hidden_ref, down_w, keep_ref):
    down_half(hidden_ref[...], lax.axis_index("core"), down_w, keep_ref)


def combine_kernel(stream_ref, combine_ref, returned_ref, out_ref):
    weight = combine_ref[...]
    high = weight.astype(BF16)
    low = (weight - high.astype(F32)).astype(BF16)
    rows = returned_ref[...]
    out_ref[...] = (stream_ref[...] + (dot(high, rows) + dot(low, rows))).astype(out_ref.dtype)


def work(macs):
    return pl.CostEstimate(flops=2 * macs, bytes_accessed=0, transcendentals=0)


def call(kernel, shapes, args, **params):
    vmem = pl.BlockSpec(memory_space=pltpu.VMEM)
    many = isinstance(shapes, (list, tuple))
    return pl.pallas_call(
        kernel,
        out_shape=shapes,
        in_specs=[vmem] * len(args),
        out_specs=[vmem] * len(shapes) if many else vmem,
        compiler_params=pltpu.CompilerParams(vmem_limit_bytes=40 * 1024 * 1024),
        **params,
    )(*args)


def attend(
    lengths,
    tokens,
    norm_gain,
    w_forget,
    w_query,
    w_key,
    w_value,
    w_output,
    key_cache,
    value_cache,
    gate_cache,
    routes,
    route_logits,
    y_count,
    ep_count,
):
    seqs, width = tokens.shape
    kv, head_dim, span = key_cache.shape[1:]
    heads = gate_cache.shape[1]
    half = width // CORES
    capacity = 2 * seqs * routes.shape[1] // ep_count
    slot_count = ep_count * capacity
    group = min(seqs, max(1, 256 // (kv * head_dim)))
    groups = seqs // group
    bounds = sorted({groups * x // SHARES[-1] for x in SHARES})
    sizes = (seqs, heads, kv, head_dim, span, group, bounds, y_count, ep_count, capacity)
    kv_width = kv * head_dim
    all_rows = seqs * heads
    shape = jax.ShapeDtypeStruct
    vmem = pl.BlockSpec(memory_space=pltpu.VMEM)
    hbm = pl.BlockSpec(memory_space=pltpu.HBM)
    forget_t = w_forget.T
    routes_t = routes.T
    return pl.pallas_call(
        functools.partial(attention_kernel, sizes),
        out_shape=[
            shape((seqs, half), F32),
            shape((seqs, half), BF16),
            shape((slot_count, seqs), BF16),
            shape((seqs, y_count * slot_count), F32),
        ],
        in_specs=[hbm] * 13,
        out_specs=[vmem] * 4,
        scratch_shapes=[
            pltpu.SMEM(lengths.shape, jnp.int32),
            pltpu.VMEM(routes_t.shape, jnp.int32),
            pltpu.VMEM(routes_t.shape, F32),
            pltpu.VMEM(tokens.shape, BF16),
            pltpu.VMEM((1, width), F32),
            pltpu.VMEM(forget_t.shape, BF16),
            pltpu.VMEM(w_query.shape, BF16),
            pltpu.VMEM(w_key.shape, BF16),
            pltpu.VMEM(w_value.shape, BF16),
            pltpu.VMEM(w_output.shape, BF16),
            pltpu.VMEM(key_cache.shape, BF16),
            pltpu.VMEM(value_cache.shape, BF16),
            pltpu.VMEM(gate_cache.shape, F32),
            pltpu.VMEM((all_rows, group * kv_width), BF16),
            pltpu.VMEM((all_rows, kv_width), BF16),
            pltpu.VMEM((all_rows, 1), F32),
            pltpu.VMEM((all_rows, 1), F32),
            pltpu.VMEM((all_rows, kv_width), F32),
            pltpu.VMEM((all_rows, span), BF16),
            pltpu.VMEM((all_rows, 1), F32),
            pltpu.VMEM((all_rows, 1), F32),
            pltpu.SemaphoreType.DMA((10,)),
            pltpu.SemaphoreType.DMA((len(bounds) - 1, 3)),
        ],
        compiler_params=pltpu.CompilerParams(vmem_limit_bytes=40 * 1024 * 1024),
        name="attend",
    )(
        *[
            pltpu.with_memory_space_constraint(x, pltpu.HBM)
            for x in (
                lengths,
                tokens,
                norm_gain.reshape(1, width),
                forget_t,
                w_query,
                w_key,
                w_value,
                w_output,
                key_cache,
                value_cache,
                gate_cache,
                routes_t,
                route_logits.T,
            )
        ]
    )


def body(
    tokens,
    norm_gain,
    post_gain,
    w_query,
    w_key,
    w_value,
    w_forget,
    w_output,
    key_cache,
    value_cache,
    gate_cache,
    lengths,
    routes,
    route_logits,
    w_gate,
    w_up,
    w_down,
):
    ep_count = lax.axis_size("ep")
    y_count = lax.axis_size("y")
    seqs, width = tokens.shape
    heads = gate_cache.shape[1]
    own_width = width // (y_count * CORES)
    half = own_width * y_count
    capacity = 2 * seqs * routes.shape[1] // ep_count
    slot_count = ep_count * capacity
    shape = jax.ShapeDtypeStruct
    keep, send, dispatch, combine = attend(
        lengths,
        tokens,
        norm_gain,
        w_forget,
        w_query,
        w_key,
        w_value,
        w_output,
        key_cache,
        value_cache,
        gate_cache,
        routes,
        route_logits,
        y_count,
        ep_count,
    )
    send, w_gate, w_up, w_down = lax.optimization_barrier((send, w_gate, w_up, w_down))
    swap = [(i, 1 - i) for i in range(CORES)]
    mine = keep + lax.ppermute(send, "core", swap).astype(F32)
    if y_count == 2:
        theirs = lax.ppermute(mine.astype(BF16), "y", [(0, 1), (1, 0)])
    else:
        parts = lax.all_gather(mine.astype(BF16), "y")
        theirs = jnp.sum(parts.astype(F32), axis=0)
        mine = jnp.zeros_like(mine)
    packed, stream = call(
        functools.partial(dispatch_kernel, y_count),
        [shape((slot_count, half), BF16), shape((seqs, own_width), F32)],
        (tokens, mine, theirs, dispatch),
        name="dispatch",
        cost_estimate=pl.CostEstimate(flops=PREFETCH_HINT, bytes_accessed=0, transcendentals=0),
    )
    arrived = lax.all_to_all(
        packed.reshape(ep_count, capacity, half), "ep", split_axis=0, concat_axis=0, tiled=True
    ).reshape(slot_count, half)
    beside = lax.ppermute(arrived, "core", swap)
    back = (ep_count, y_count, capacity, own_width)
    hidden_shape = (slot_count, w_gate.shape[2])
    gain = post_gain.reshape(1, width)
    halves = call(
        functools.partial(first_half_kernel, y_count),
        [shape((slot_count, 1), F32), shape(hidden_shape, F32), shape(hidden_shape, F32)],
        (arrived, gain, w_gate, w_up, w_down),
        name="first_half",
        cost_estimate=work(slot_count * half * 2 * hidden_shape[1]),
    )
    hidden, send = call(
        second_half_kernel,
        [shape(hidden_shape, BF16), shape(back, BF16)],
        (beside, *halves, gain, w_gate, w_up, w_down),
        name="second_half",
        cost_estimate=work(slot_count * half * 3 * hidden_shape[1]),
    )
    arriving = lax.ppermute(send, "core", swap)
    keep = call(
        keep_kernel,
        shape(back, F32),
        (hidden, w_down),
        name="keep",
        cost_estimate=work(slot_count * half * hidden_shape[1]),
    )
    summed = (keep + arriving.astype(F32)).astype(BF16)
    returned = lax.all_to_all(
        summed.reshape(ep_count * y_count, capacity, own_width),
        ("ep", "y"),
        split_axis=0,
        concat_axis=0,
        tiled=True,
    ).reshape(ep_count * y_count * capacity, own_width)
    return call(
        combine_kernel,
        shape((seqs, own_width), BF16),
        (stream, combine, returned),
        name="combine",
    )


def solution(mesh):
    ep_count, tp_count = mesh.devices.shape
    inner = Mesh(
        mesh.devices.reshape(ep_count, tp_count // CORES, CORES), ("ep", "y", "core")
    )
    tp = ("y", "core")
    in_specs = (
        P("ep", None),
        P(),
        P(),
        P(None, tp),
        P(None, tp),
        P(None, tp),
        P(),
        P(tp, None),
        P("ep", tp, None, None),
        P("ep", tp, None, None),
        P("ep", tp, None),
        P("ep"),
        P("ep", None),
        P("ep", None),
        P("ep", None, tp),
        P("ep", None, tp),
        P("ep", tp, None),
    )
    return jax.shard_map(
        body, mesh=inner, in_specs=in_specs, out_specs=P("ep", tp), check_vma=False
    )
```

```python
import functools
import itertools

import jax
import jax.numpy as jnp
from jax import lax
from jax.experimental import pallas as pl
from jax.experimental.pallas import tpu as pltpu
from jax.sharding import Mesh
from jax.sharding import PartitionSpec as P

epsilon = 1e-06
CORES = 2
SHARES = (0, 5, 9, 12, 14, 16)
AHEAD = 3
PREFETCH_HINT = 10**11
F32 = jnp.float32
BF16 = jnp.bfloat16
NT = (((1,), (1,)), ((), ()))


def log2(n):
    assert n & (n - 1) == 0
    return n.bit_length() - 1


def dot(a, b):
    return jnp.dot(a, b, preferred_element_type=F32)


def iota(shape, axis):
    return lax.broadcasted_iota(jnp.int32, shape, axis)


def attention_kernel(
    sizes,
    lengths_hbm,
    tokens_hbm,
    gain_hbm,
    forget_hbm,
    query_hbm,
    key_w_hbm,
    value_w_hbm,
    out_w_hbm,
    key_hbm,
    value_hbm,
    gate_hbm,
    routes_hbm,
    logits_hbm,
    keep_ref,
    send_ref,
    dispatch_ref,
    combine_ref,
    lengths_ref,
    routes_ref,
    logits_ref,
    tokens_ref,
    gain_ref,
    forget_ref,
    query_w,
    key_w,
    value_w,
    out_w,
    keys,
    values,
    gates,
    wide_query,
    mixed,
    forget_col,
    new_col,
    new_value,
    probs,
    new_exps,
    totals,
    first_sems,
    cache_sems,
):
    seqs, heads, kv, head_dim, span, group, bounds, y_count, ep_count, capacity = sizes
    groups = seqs // group
    rows = group * heads
    kv_width = kv * head_dim
    head_width = heads * head_dim
    firsts = [
        (tokens_hbm, tokens_ref),
        (gain_hbm, gain_ref),
        (forget_hbm, forget_ref),
        (query_hbm, query_w),
        (key_w_hbm, key_w),
        (value_w_hbm, value_w),
        (lengths_hbm, lengths_ref),
        (routes_hbm, routes_ref),
        (logits_hbm, logits_ref),
        (out_w_hbm, out_w),
    ]
    copies = [
        pltpu.make_async_copy(src, dst, first_sems.at[i]) for i, (src, dst) in enumerate(firsts)
    ]

    caches = ((key_hbm, keys), (gate_hbm, gates), (value_hbm, values))

    chunks = len(bounds) - 1

    def cache_copy(c, i):
        part = pl.ds(bounds[c] * group, (bounds[c + 1] - bounds[c]) * group)
        src, dst = caches[i]
        return pltpu.make_async_copy(src.at[part], dst.at[part], cache_sems.at[c, i])

    def start_chunk(c):
        if c < chunks:
            for i in range(3):
                cache_copy(c, i).start()
        elif c == chunks:
            copies[-1].start()

    for c in copies[:-1]:
        c.start()
    start_chunk(0)

    core = lax.axis_index("core")
    head_start = (lax.axis_index("y") * CORES + core) * heads

    for c in copies[:-1]:
        c.wait()
    for c in range(1, AHEAD):
        start_chunk(c)

    experts = iota((ep_count, seqs), 0)
    picks = [routes_ref[k : k + 1, :] for k in range(2)]
    named = jnp.zeros((ep_count, seqs), F32)
    for k in range(2):
        named = named + (experts == picks[k]).astype(F32)
    earlier = (iota((seqs, seqs), 0) < iota((seqs, seqs), 1)).astype(BF16)
    rank = dot(named.astype(BF16), earlier)
    slot_of = experts.astype(F32) * capacity + rank
    slots = [
        jnp.sum(jnp.where(experts == picks[k], slot_of, 0.0), axis=0, keepdims=True)
        for k in range(2)
    ]
    slot_iota = iota((ep_count * capacity, seqs), 0).astype(F32)
    dispatch_ref[...] = jnp.logical_or(slot_iota == slots[0], slot_iota == slots[1]).astype(
        F32
    ).astype(BF16)
    logits = [logits_ref[k : k + 1, :] for k in range(2)]
    top = jnp.maximum(logits[0], logits[1])
    raised = [jnp.exp(x - top) for x in logits]
    total = raised[0] + raised[1]
    eye = iota((seqs, seqs), 0) == iota((seqs, seqs), 1)

    def column(x):
        return jnp.sum(jnp.where(eye, x, 0.0), axis=1, keepdims=True)

    returned = (seqs, ep_count * y_count * capacity)
    back = iota(returned, 1)
    back_slot = jnp.bitwise_and(back, (1 << log2(ep_count * capacity)) - 1).astype(F32)
    combine_ref[...] = jnp.where(
        back_slot == column(slots[0]), column(raised[0] / total), 0.0
    ) + jnp.where(back_slot == column(slots[1]), column(raised[1] / total), 0.0)

    wide = tokens_ref[...].astype(F32)
    normed = (
        wide
        * lax.rsqrt(jnp.mean(wide * wide, axis=-1, keepdims=True) + epsilon)
        * gain_ref[...]
    ).astype(BF16)
    all_rows = (seqs * heads, seqs)
    repeat = (lax.shift_right_logical(iota(all_rows, 0), log2(heads)) == iota(all_rows, 1)).astype(
        F32
    )
    repeat_b = repeat.astype(BF16)
    forget_logit = lax.dot_general(normed, forget_ref[...], NT, preferred_element_type=F32)
    log_forget = jax.nn.log_sigmoid(forget_logit)
    spread = jnp.dot(repeat, log_forget, precision=lax.Precision.HIGHEST, preferred_element_type=F32)
    head_of_row = jnp.bitwise_and(iota(spread.shape, 0), heads - 1)
    forget_col[...] = jnp.sum(
        jnp.where(iota(spread.shape, 1) == head_of_row + head_start, spread, 0.0),
        axis=1,
        keepdims=True,
    )
    query = dot(normed, query_w[...]).astype(BF16)
    fresh_key = dot(normed, key_w[...]).astype(BF16)
    fresh_value = dot(normed, value_w[...]).astype(BF16)
    wide_shape = (seqs * heads, head_width)
    own_head = lax.shift_right_logical(iota(wide_shape, 1), log2(head_dim)) == jnp.bitwise_and(
        iota(wide_shape, 0), heads - 1
    )
    fold_shape = (head_width, kv_width)
    fold_row = iota(fold_shape, 0)
    fold = (
        iota(fold_shape, 1)
        == lax.shift_right_logical(fold_row, log2(heads // kv * head_dim)) * head_dim
        + jnp.bitwise_and(fold_row, head_dim - 1)
    ).astype(F32).astype(BF16)
    spread_query = jnp.where(own_head, dot(repeat_b, query), 0.0).astype(BF16)
    folded = dot(spread_query, fold)
    member = jnp.bitwise_and(
        lax.shift_right_logical(iota(folded.shape, 0), log2(heads)), group - 1
    )
    for m in range(group):
        wide_query[:, m * kv_width : (m + 1) * kv_width] = jnp.where(
            member == m, folded, 0.0
        ).astype(BF16)
    scale = head_dim ** (-0.5)
    new_col[...] = (
        jnp.sum(folded * dot(repeat_b, fresh_key), axis=1, keepdims=True) * scale
    )
    new_value[...] = dot(repeat_b, fresh_value)

    position = iota((rows, span), 1)
    row_member = lax.shift_right_logical(iota((rows, span), 0), log2(heads))
    small_member = lax.shift_right_logical(iota((rows, kv_width), 0), log2(heads))

    def scores(g):
        at = slice(g * rows, (g + 1) * rows)
        part = slice(g * group, (g + 1) * group)
        raw = dot(wide_query[at, :], keys[part].reshape(group * kv_width, span))
        gate = gates[part].reshape(rows, span)
        length = jnp.full((rows, span), lengths_ref[g * group], jnp.int32)
        for m in range(1, group):
            length = jnp.where(row_member == m, lengths_ref[g * group + m], length)
        latest = jnp.sum(
            jnp.where(position == length - 1, gate, 0.0), axis=1, keepdims=True
        )
        past = raw * scale + (latest + forget_col[at, :]) - gate
        past = jnp.where(position < length, past, -jnp.inf)
        fresh = new_col[at, :]
        peak = jnp.maximum(jnp.max(past, axis=1, keepdims=True), fresh)
        past_exp = jnp.exp(past - peak)
        new_exp = jnp.exp(fresh - peak)
        total = jnp.sum(past_exp, axis=1, keepdims=True) + new_exp
        probs[at, :] = past_exp.astype(BF16)
        new_exps[at, :] = new_exp
        totals[at, :] = total

    def mix(g):
        at = slice(g * rows, (g + 1) * rows)
        part = slice(g * group, (g + 1) * group)
        out = lax.dot_general(
            probs[at, :],
            values[part].reshape(group * kv_width, span),
            NT,
            preferred_element_type=F32,
        )
        own = jnp.zeros((rows, kv_width), F32)
        for m in range(group):
            own = jnp.where(small_member == m, out[:, m * kv_width : (m + 1) * kv_width], own)
        mixed[at, :] = ((own + new_exps[at, :] * new_value[at, :]) / totals[at, :]).astype(BF16)

    for c in range(chunks + 1):
        if c < chunks:
            cache_copy(c, 0).wait()
            cache_copy(c, 1).wait()
        if c > 0:
            cache_copy(c - 1, 2).wait()
        start_chunk(c + AHEAD)
        new = range(bounds[c], bounds[c + 1]) if c < chunks else ()
        old = range(bounds[c - 1], bounds[c]) if c > 0 else ()
        for g, h in itertools.zip_longest(new, old):
            if g is not None:
                scores(g)
            if h is not None:
                mix(h)

    unfolded = lax.dot_general(mixed[...], fold, NT, preferred_element_type=F32)
    unfolded = jnp.where(own_head, unfolded, 0.0).astype(BF16)
    gather_shape = (seqs, seqs * heads)
    gather = (
        lax.shift_right_logical(iota(gather_shape, 1), log2(heads)) == iota(gather_shape, 0)
    ).astype(F32).astype(BF16)
    attended = dot(gather, unfolded).astype(BF16)
    copies[-1].wait()
    own_width = keep_ref.shape[1] // y_count
    for y in range(y_count):
        at = slice(y * own_width, (y + 1) * own_width)
        for ref, which in ((send_ref, 1 - core), (keep_ref, core)):
            start = pl.multiple_of((y * CORES + which) * own_width, own_width)
            ref[:, at] = dot(attended, out_w[:, pl.ds(start, own_width)]).astype(ref.dtype)


def dispatch_kernel(
    y_count, tokens_ref, mine_ref, theirs_ref, dispatch_ref, packed_ref, own_ref
):
    core = lax.axis_index("core")
    y_index = lax.axis_index("y")
    own_width = own_ref.shape[1]
    for y in range(y_count):
        at = slice(y * own_width, (y + 1) * own_width)
        start = pl.multiple_of((y * CORES + core) * own_width, own_width)
        attention = mine_ref[:, at] + theirs_ref[:, at].astype(F32)
        stream = tokens_ref[:, pl.ds(start, own_width)].astype(F32) + attention
        packed_ref[:, at] = dot(dispatch_ref[...], stream.astype(BF16)).astype(BF16)

        @pl.when(y_index == y)
        def _():
            own_ref[...] = stream


def half_products(rows_ref, which, y_count, gain_ref, gate_w, up_w):
    own_width = rows_ref.shape[1] // y_count
    squares, gate_act, upper = 0.0, 0.0, 0.0
    for y in range(y_count):
        start = pl.multiple_of((y * CORES + which) * own_width, own_width)
        part = pl.ds(start, own_width)
        x = rows_ref[:, y * own_width : (y + 1) * own_width].astype(F32)
        squares = squares + jnp.sum(x * x, axis=1, keepdims=True)
        x = (x * gain_ref[:, part]).astype(BF16)
        gate_act = gate_act + dot(x, gate_w[0, part, :])
        upper = upper + dot(x, up_w[0, part, :])
    return squares, gate_act, upper


def first_half_kernel(
    y_count, mine_ref, gain_ref, gate_w, up_w, down_w, squares_ref, gate_ref, upper_ref
):
    del down_w
    squares_ref[...], gate_ref[...], upper_ref[...] = half_products(
        mine_ref, lax.axis_index("core"), y_count, gain_ref, gate_w, up_w
    )


def down_half(hidden, which, down_w, ref):
    y_count, _, own_width = ref.shape
    for y in range(y_count):
        start = pl.multiple_of((y * CORES + which) * own_width, own_width)
        ref[y] = dot(hidden, down_w[0, :, pl.ds(start, own_width)]).astype(ref.dtype)


def second_half_kernel(
    theirs_ref,
    squares_ref,
    gate_ref,
    upper_ref,
    gain_ref,
    gate_w,
    up_w,
    down_w,
    hidden_ref,
    send_ref,
):
    other = 1 - lax.axis_index("core")
    y_count = send_ref.shape[0]
    width = theirs_ref.shape[1] * CORES
    squares, gate_act, upper = half_products(
        theirs_ref, other, y_count, gain_ref, gate_w, up_w
    )
    inverse = lax.rsqrt((squares + squares_ref[...]) / width + epsilon)
    gate_act = (gate_act + gate_ref[...]) * inverse
    upper = (upper + upper_ref[...]) * inverse
    hidden = (gate_act / (1.0 + jnp.exp(-gate_act)) * upper).astype(BF16)
    hidden_ref[...] = hidden
    down_half(hidden, other, down_w, send_ref)


def keep_kernel(hidden_ref, down_w, keep_ref):
    down_half(hidden_ref[...], lax.axis_index("core"), down_w, keep_ref)


def combine_kernel(stream_ref, combine_ref, returned_ref, out_ref):
    weight = combine_ref[...]
    high = weight.astype(BF16)
    low = (weight - high.astype(F32)).astype(BF16)
    count = high.shape[0]
    mixed = dot(jnp.concatenate([high, low], axis=0), returned_ref[...])
    out_ref[...] = (stream_ref[...] + (mixed[:count] + mixed[count:])).astype(out_ref.dtype)


def work(macs):
    return pl.CostEstimate(flops=2 * macs, bytes_accessed=0, transcendentals=0)


def call(kernel, shapes, args, **params):
    vmem = pl.BlockSpec(memory_space=pltpu.VMEM)
    many = isinstance(shapes, (list, tuple))
    return pl.pallas_call(
        kernel,
        out_shape=shapes,
        in_specs=[vmem] * len(args),
        out_specs=[vmem] * len(shapes) if many else vmem,
        compiler_params=pltpu.CompilerParams(vmem_limit_bytes=40 * 1024 * 1024),
        **params,
    )(*args)


def attend(
    lengths,
    tokens,
    norm_gain,
    w_forget,
    w_query,
    w_key,
    w_value,
    w_output,
    key_cache,
    value_cache,
    gate_cache,
    routes,
    route_logits,
    y_count,
    ep_count,
):
    seqs, width = tokens.shape
    kv, head_dim, span = key_cache.shape[1:]
    heads = gate_cache.shape[1]
    half = width // CORES
    capacity = 2 * seqs * routes.shape[1] // ep_count
    slot_count = ep_count * capacity
    group = min(seqs, max(1, 256 // (kv * head_dim)))
    groups = seqs // group
    bounds = sorted({groups * x // SHARES[-1] for x in SHARES})
    sizes = (seqs, heads, kv, head_dim, span, group, bounds, y_count, ep_count, capacity)
    kv_width = kv * head_dim
    all_rows = seqs * heads
    shape = jax.ShapeDtypeStruct
    vmem = pl.BlockSpec(memory_space=pltpu.VMEM)
    hbm = pl.BlockSpec(memory_space=pltpu.HBM)
    forget_t = w_forget.T
    routes_t = routes.T
    return pl.pallas_call(
        functools.partial(attention_kernel, sizes),
        out_shape=[
            shape((seqs, half), F32),
            shape((seqs, half), BF16),
            shape((slot_count, seqs), BF16),
            shape((seqs, y_count * slot_count), F32),
        ],
        in_specs=[hbm] * 13,
        out_specs=[vmem] * 4,
        scratch_shapes=[
            pltpu.SMEM(lengths.shape, jnp.int32),
            pltpu.VMEM(routes_t.shape, jnp.int32),
            pltpu.VMEM(routes_t.shape, F32),
            pltpu.VMEM(tokens.shape, BF16),
            pltpu.VMEM((1, width), F32),
            pltpu.VMEM(forget_t.shape, BF16),
            pltpu.VMEM(w_query.shape, BF16),
            pltpu.VMEM(w_key.shape, BF16),
            pltpu.VMEM(w_value.shape, BF16),
            pltpu.VMEM(w_output.shape, BF16),
            pltpu.VMEM(key_cache.shape, BF16),
            pltpu.VMEM(value_cache.shape, BF16),
            pltpu.VMEM(gate_cache.shape, F32),
            pltpu.VMEM((all_rows, group * kv_width), BF16),
            pltpu.VMEM((all_rows, kv_width), BF16),
            pltpu.VMEM((all_rows, 1), F32),
            pltpu.VMEM((all_rows, 1), F32),
            pltpu.VMEM((all_rows, kv_width), F32),
            pltpu.VMEM((all_rows, span), BF16),
            pltpu.VMEM((all_rows, 1), F32),
            pltpu.VMEM((all_rows, 1), F32),
            pltpu.SemaphoreType.DMA((10,)),
            pltpu.SemaphoreType.DMA((len(bounds) - 1, 3)),
        ],
        compiler_params=pltpu.CompilerParams(vmem_limit_bytes=40 * 1024 * 1024),
        name="attend",
    )(
        *[
            pltpu.with_memory_space_constraint(x, pltpu.HBM)
            for x in (
                lengths,
                tokens,
                norm_gain.reshape(1, width),
                forget_t,
                w_query,
                w_key,
                w_value,
                w_output,
                key_cache,
                value_cache,
                gate_cache,
                routes_t,
                route_logits.T,
            )
        ]
    )


def body(
    tokens,
    norm_gain,
    post_gain,
    w_query,
    w_key,
    w_value,
    w_forget,
    w_output,
    key_cache,
    value_cache,
    gate_cache,
    lengths,
    routes,
    route_logits,
    w_gate,
    w_up,
    w_down,
):
    ep_count = lax.axis_size("ep")
    y_count = lax.axis_size("y")
    seqs, width = tokens.shape
    heads = gate_cache.shape[1]
    own_width = width // (y_count * CORES)
    half = own_width * y_count
    capacity = 2 * seqs * routes.shape[1] // ep_count
    slot_count = ep_count * capacity
    shape = jax.ShapeDtypeStruct
    keep, send, dispatch, combine = attend(
        lengths,
        tokens,
        norm_gain,
        w_forget,
        w_query,
        w_key,
        w_value,
        w_output,
        key_cache,
        value_cache,
        gate_cache,
        routes,
        route_logits,
        y_count,
        ep_count,
    )
    send, w_gate, w_up, w_down = lax.optimization_barrier((send, w_gate, w_up, w_down))
    swap = [(i, 1 - i) for i in range(CORES)]
    mine = keep + lax.ppermute(send, "core", swap).astype(F32)
    if y_count == 2:
        theirs = lax.ppermute(mine.astype(BF16), "y", [(0, 1), (1, 0)])
    else:
        parts = lax.all_gather(mine.astype(BF16), "y")
        theirs = jnp.sum(parts.astype(F32), axis=0)
        mine = jnp.zeros_like(mine)
    packed, stream = call(
        functools.partial(dispatch_kernel, y_count),
        [shape((slot_count, half), BF16), shape((seqs, own_width), F32)],
        (tokens, mine, theirs, dispatch),
        name="dispatch",
        cost_estimate=pl.CostEstimate(flops=PREFETCH_HINT, bytes_accessed=0, transcendentals=0),
    )
    arrived = lax.all_to_all(
        packed.reshape(ep_count, capacity, half), "ep", split_axis=0, concat_axis=0, tiled=True
    ).reshape(slot_count, half)
    beside = lax.ppermute(arrived, "core", swap)
    back = (y_count, slot_count, own_width)
    hidden_shape = (slot_count, w_gate.shape[2])
    gain = post_gain.reshape(1, width)
    halves = call(
        functools.partial(first_half_kernel, y_count),
        [shape((slot_count, 1), F32), shape(hidden_shape, F32), shape(hidden_shape, F32)],
        (arrived, gain, w_gate, w_up, w_down),
        name="first_half",
        cost_estimate=work(slot_count * half * 2 * hidden_shape[1]),
    )
    hidden, send = call(
        second_half_kernel,
        [shape(hidden_shape, BF16), shape(back, BF16)],
        (beside, *halves, gain, w_gate, w_up, w_down),
        name="second_half",
        cost_estimate=work(slot_count * half * 3 * hidden_shape[1]),
    )
    arriving = lax.ppermute(send, "core", swap)
    keep = call(
        keep_kernel,
        shape(back, F32),
        (hidden, w_down),
        name="keep",
        cost_estimate=work(slot_count * half * hidden_shape[1]),
    )
    summed = (keep + arriving.astype(F32)).astype(BF16)
    returned = lax.all_to_all(
        summed.reshape(y_count * ep_count, capacity, own_width),
        ("y", "ep"),
        split_axis=0,
        concat_axis=0,
        tiled=True,
    ).reshape(y_count * slot_count, own_width)
    return call(
        combine_kernel,
        shape((seqs, own_width), BF16),
        (stream, combine, returned),
        name="combine",
    )


def solution(mesh):
    ep_count, tp_count = mesh.devices.shape
    inner = Mesh(
        mesh.devices.reshape(ep_count, tp_count // CORES, CORES), ("ep", "y", "core")
    )
    tp = ("y", "core")
    in_specs = (
        P("ep", None),
        P(),
        P(),
        P(None, tp),
        P(None, tp),
        P(None, tp),
        P(),
        P(tp, None),
        P("ep", tp, None, None),
        P("ep", tp, None, None),
        P("ep", tp, None),
        P("ep"),
        P("ep", None),
        P("ep", None),
        P("ep", None, tp),
        P("ep", None, tp),
        P("ep", tp, None),
    )
    return jax.shard_map(
        body, mesh=inner, in_specs=in_specs, out_specs=P("ep", tp), check_vma=False
    )
```
